768 devices in a mesh: sp: 192 (over z, y, core), tp: 4 (over x).
Axes of the slice: x: 4, y: 8, z: 12, core: 2. Of those that a mesh axis runs over, the one named last changes fastest.
Arguments:
- query_latent: bfloat16 [49152, 1024], P('sp'), may hold values from -6 to 6
- shared_latent: bfloat16 [49152, 512], P('sp'), may hold values from -25 to 25
- rotary_key: bfloat16 [49152, 64], P('sp'), may hold values from -300 to 300
- document_start: int32 [49152], P('sp'), may hold values from 0 to 49151, as said below
- query_gain: float32 [1024], replicated, may hold values from 0.1 to 1.9
- shared_gain: float32 [512], replicated, may hold values from 0.1 to 1.9
- content_weight: bfloat16 [1024, 2048], P(None, 'tp'), may hold values from -0.1875 to 0.1875
- rotary_weight: bfloat16 [1024, 1024], P(None, 'tp'), may hold values from -0.1875 to 0.1875
- key_weight: bfloat16 [512, 2048], P(None, 'tp'), may hold values from -0.25 to 0.25
- value_weight: bfloat16 [512, 2048], P(None, 'tp'), may hold values from -0.25 to 0.25
- output_weight: bfloat16 [2048, 4096], P('tp'), may hold values from -0.125 to 0.125
Outputs:
- mixed: bfloat16 [49152, 4096], P('sp')
The draws below stay inside these ranges and needn't reach their ends.
Inputs may be any that keep to these rules, and one draw needn't show every extreme that they name: `document_start`: each position holds the first position of its document; documents are runs of 1 to 1792 consecutive positions and one of them has exactly 1792; the values never fall.
All inputs are finite; a program needn't handle non-finite values.
Results may differ from the reference program's by a relative error of at most 0.038.
The reference program's roundings to bfloat16 on the way count: a program that leaves them out, or rounds other values in their place, can miss the bound.
Values may be sent and summed in bfloat16 or wider, within the bound.
A program may use at most 64 MiB of HBM per device.

```python
import jax
import jax.numpy as jnp
from jax import lax

MODEL = 4096
HEADS = 16
CONTENT = 128
ROTARY = 64
VALUE_DIM = 128
QUERY_RANK = 1024
SHARED_RANK = 512
SPAN = 8
TOK_DEV = 256
TOKENS = 49152
DOC_MOST = 1792
HEADS_DEV = 4


def draw_shared_latent(key, part):
    first_key = jax.random.fold_in(key, 11)
    second_key = jax.random.fold_in(key, 12)
    blocks = TOKENS // TOK_DEV
    base = jnp.clip(jax.random.normal(first_key, (TOKENS, SHARED_RANK), jnp.float32), -6.0, 6.0)
    means = 0.8 * jnp.clip(jax.random.normal(second_key, (blocks, SHARED_RANK), jnp.float32), -6.0, 6.0)
    result = base + jnp.repeat(means, TOK_DEV, axis=0)
    return jnp.clip(result, -25.0, 25.0).astype(jnp.bfloat16)


def draw_rotary_key(key, part):
    first_key = jax.random.fold_in(key, 21)
    result = jnp.clip(jax.random.normal(first_key, (TOKENS, ROTARY), jnp.float32), -6.0, 6.0)
    return jnp.clip(result, -300.0, 300.0).astype(jnp.bfloat16)


def draw_document_start(key, part):
    first_key = jax.random.fold_in(key, 31)
    second_key = jax.random.fold_in(key, 32)
    positions = jnp.arange(TOKENS, dtype=jnp.int32)
    lengths = jax.random.randint(first_key, (TOKENS,), 1, DOC_MOST + 1, dtype=jnp.int32)
    opening = jax.random.randint(second_key, (), 1, TOK_DEV, dtype=jnp.int32)
    lengths = jnp.where(positions == 0, opening, jnp.where(positions == 1, DOC_MOST, lengths))
    starts = jnp.cumsum(lengths).astype(jnp.int32) - lengths
    document = jnp.searchsorted(starts, positions, side='right') - 1
    result = starts[document].astype(jnp.int32)
    return jnp.where(positions == TOKENS - 1, positions, result).astype(jnp.int32)


def block_scale(key, shape, shards, low, largest):
    factor_of, own = 1.0, jax.random.fold_in(key, 6)
    for position, shards_of in shards:
        draws = jnp.exp(jax.random.uniform(jax.random.fold_in(own, position), (shards_of,), jnp.float32, low / len(shards), largest / len(shards)))
        factor_of = factor_of * jnp.repeat(draws, shape[position] // shards_of).reshape([-1 if axis == position else 1 for axis in range(len(shape))])
    return factor_of


def bell_draw(rng, extent, scale, bound, pieces=(), held_as=jnp.bfloat16):
    values = jax.random.normal(rng, extent, jnp.float32) * scale
    if len(pieces) > 0:
        values = block_scale(rng, extent, pieces, -0.22, 0.18) * values
    return jnp.clip(values, min=-bound, max=bound).astype(held_as)


def setup_inputs(seed: int = 0) -> dict:
    arg_keys = jax.random.split(jax.random.key(seed), 12)
    return {
        "query_latent": bell_draw(arg_keys[0], (TOKENS, QUERY_RANK), 1.0, 6.0, ((0, 192),)),
        "shared_latent": draw_shared_latent(jax.random.fold_in(arg_keys[11], 71), 0),
        "rotary_key": draw_rotary_key(jax.random.fold_in(arg_keys[11], 71), 0),
        "document_start": draw_document_start(jax.random.fold_in(arg_keys[11], 71), 0),
        "query_gain": jnp.clip(1.0 + 0.18 * jax.random.normal(arg_keys[4], (QUERY_RANK,), jnp.float32), 0.1, 1.9),
        "shared_gain": jnp.clip(1.0 + 0.18 * jax.random.normal(arg_keys[5], (SHARED_RANK,), jnp.float32), 0.1, 1.9),
        "content_weight": bell_draw(arg_keys[6], (QUERY_RANK, HEADS * CONTENT), QUERY_RANK ** -0.5, 0.1875, ((1, 4),)),
        "rotary_weight": bell_draw(arg_keys[7], (QUERY_RANK, HEADS * ROTARY), QUERY_RANK ** -0.5, 0.1875, ((1, 4),)),
        "key_weight": bell_draw(arg_keys[8], (SHARED_RANK, HEADS * CONTENT), SHARED_RANK ** -0.5, 0.25, ((1, 4),)),
        "value_weight": bell_draw(arg_keys[9], (SHARED_RANK, HEADS * VALUE_DIM), SHARED_RANK ** -0.5, 0.25, ((1, 4),)),
        "output_weight": bell_draw(arg_keys[10], (HEADS * VALUE_DIM, MODEL), (HEADS * VALUE_DIM) ** -0.5, 0.125, ((0, 4),)),
    }


norm_eps = 1e-06
rope_theta = 10000.0
masked_score = -1e+30

def rms_scale(latent, scaling):
    entries = latent.astype(jnp.float32)
    scaled = entries * lax.rsqrt(lax.optimization_barrier(jnp.mean(entries * entries, axis=-1, keepdims=True)) + norm_eps)
    return (scaled * scaling.astype(jnp.float32)).astype(jnp.bfloat16)

def rotate(entries, places):
    width = entries.shape[-1]
    halfway = width // 2
    frequency = 1.0 / rope_theta ** (jnp.arange(0, width, 2, dtype=jnp.float32) / width)
    angles = places.astype(jnp.float32)[:, None] * frequency[None, :]
    target = (angles.shape[0],) + (1,) * (entries.ndim - 2) + (halfway,)
    cosine_table = jnp.cos(angles).reshape(target)
    sine_table = jnp.sin(angles).reshape(target)
    leading = entries[..., :halfway]
    trailing = entries[..., halfway:]
    return jnp.concatenate([leading * cosine_table - trailing * sine_table, leading * sine_table + trailing * cosine_table], axis=-1)

def reference(query_latent, shared_latent, rotary_key, document_start, query_gain, shared_gain, content_weight, rotary_weight, key_weight, value_weight, output_weight):
    places = jnp.arange(TOKENS, dtype=jnp.int32)
    query_norm = rms_scale(query_latent, query_gain)
    shared_norm = rms_scale(shared_latent, shared_gain)
    key_turn = rotate(rotary_key.astype(jnp.float32), places).astype(jnp.bfloat16)
    query_content = jnp.dot(query_norm, content_weight, preferred_element_type=jnp.float32).astype(jnp.bfloat16).reshape(TOKENS, HEADS, CONTENT)
    query_raw = jnp.dot(query_norm, rotary_weight, preferred_element_type=jnp.float32).reshape(TOKENS, HEADS, ROTARY)
    query_turn = rotate(query_raw, places).astype(jnp.bfloat16)
    head_keys = jnp.dot(shared_norm, key_weight, preferred_element_type=jnp.float32).astype(jnp.bfloat16).reshape(TOKENS, HEADS, CONTENT)
    head_values = jnp.dot(shared_norm, value_weight, preferred_element_type=jnp.float32).astype(jnp.bfloat16).reshape(TOKENS, HEADS, VALUE_DIM)
    leading_pad = (SPAN - 1) * TOK_DEV
    window = SPAN * TOK_DEV
    padded_keys = jnp.pad(head_keys, ((leading_pad, 0), (0, 0), (0, 0)))
    padded_values = jnp.pad(head_values, ((leading_pad, 0), (0, 0), (0, 0)))
    padded_turn = jnp.pad(key_turn, ((leading_pad, 0), (0, 0)))
    score_scale = (CONTENT + ROTARY) ** (-0.5)

    def attend(block):
        opening = (block * TOK_DEV).astype(jnp.int32)
        block_content = lax.dynamic_slice_in_dim(query_content, opening, TOK_DEV, 0).astype(jnp.float32)
        block_turn = lax.dynamic_slice_in_dim(query_turn, opening, TOK_DEV, 0).astype(jnp.float32)
        block_starts = lax.dynamic_slice_in_dim(document_start, opening, TOK_DEV, 0)
        window_keys = lax.dynamic_slice_in_dim(padded_keys, opening, window, 0).astype(jnp.float32)
        window_values = lax.dynamic_slice_in_dim(padded_values, opening, window, 0).astype(jnp.float32)
        window_turn = lax.dynamic_slice_in_dim(padded_turn, opening, window, 0).astype(jnp.float32)
        key_places = opening - leading_pad + jnp.arange(window, dtype=jnp.int32)
        query_places = opening + jnp.arange(TOK_DEV, dtype=jnp.int32)
        scores = jnp.einsum('qhd,khd->hqk', block_content, window_keys) + jnp.einsum('qhr,kr->hqk', block_turn, window_turn)
        visible = (key_places[None, :] >= block_starts[:, None]) & (key_places[None, :] <= query_places[:, None])
        scores = jnp.where(visible[None], scores * score_scale, masked_score)
        highest = lax.optimization_barrier(jnp.max(scores, axis=-1, keepdims=True))
        weights = jnp.exp(scores - highest)
        denominator = lax.optimization_barrier(jnp.sum(weights, axis=-1))
        weights_low = weights.astype(jnp.bfloat16).astype(jnp.float32)
        summed = jnp.einsum('hqk,khd->qhd', weights_low, window_values)
        attended = summed / jnp.transpose(denominator)[:, :, None]
        return attended.astype(jnp.bfloat16).reshape(TOK_DEV, HEADS * VALUE_DIM)
    blocks = jnp.arange(TOKENS // TOK_DEV, dtype=jnp.int32)
    attended = lax.map(attend, blocks).reshape(TOKENS, HEADS * VALUE_DIM)
    group_width = HEADS_DEV * VALUE_DIM
    mixed = jnp.zeros((TOKENS, MODEL), jnp.float32)
    for group in range(HEADS // HEADS_DEV):
        columns = attended[:, group * group_width:(group + 1) * group_width]
        matching = output_weight[group * group_width:(group + 1) * group_width]
        group_term = jnp.dot(columns, matching, preferred_element_type=jnp.float32).astype(jnp.bfloat16)
        mixed = mixed + group_term.astype(jnp.float32)
    return mixed.astype(jnp.bfloat16)
```

```python
import functools

import jax
import jax.numpy as jnp
from jax import lax
from jax.experimental import pallas as pl
from jax.experimental.pallas import tpu as pltpu
from jax.sharding import PartitionSpec as P

MESH = pl.DeviceIdType.MESH
CONTENT = 128
ROTARY = 64
SPAN = 8
NORM_EPS = 1e-06
THETA = 10000.0
MASKED = -1e30
LOG2E = 1.4426950408889634
F32 = jnp.float32
BF16 = jnp.bfloat16
WHOLE = pl.BlockSpec(memory_space=pltpu.VMEM)


def copy_to(src, dst, send, recv, sp, tp):
    return pltpu.make_async_remote_copy(
        src_ref=src,
        dst_ref=dst,
        send_sem=send,
        recv_sem=recv,
        device_id={"sp": sp, "tp": tp},
        device_id_type=MESH,
    )


def rms_scale(entries, gain):
    entries = entries.astype(F32)
    mean = jnp.mean(entries * entries, axis=-1, keepdims=True)
    return (entries * lax.rsqrt(mean + NORM_EPS) * gain).astype(BF16)


def rotate(entries, cosine, sine):
    width = entries.shape[-1]
    lane = lax.broadcasted_iota(jnp.int32, entries.shape, 1)
    ahead = pltpu.roll(entries, width - ROTARY // 2, 1)
    behind = pltpu.roll(entries, ROTARY // 2, 1)
    other = jnp.where(lane % ROTARY < ROTARY // 2, ahead, behind)
    return entries * cosine + other * sine


def payload_kernel(shared_ref, rotary_ref, cos_ref, sin_ref, gain_ref, out_ref):
    rank = shared_ref.shape[1]
    out_ref[:, :rank] = rms_scale(shared_ref[...], gain_ref[...])
    turned = rotate(rotary_ref[...].astype(F32), cos_ref[...], sin_ref[...])
    out_ref[:, rank:] = turned.astype(BF16)


def exchange_kernel(
    pay_ref, win_ref, own_sem, y_send, y_recv, x_send, x_recv, d_send, d_recv
):
    count = lax.axis_size("sp")
    ring = lax.axis_size("tp")
    me = lax.axis_index("sp")
    col = lax.axis_index("tp")
    core = lax.rem(me, 2)
    sibling = me + 1 - 2 * core
    east = lax.rem(col + 1, ring)
    west = lax.rem(col + ring - 1, ring)
    length = pay_ref.shape[0]
    quarter = length // 4
    eighth = length // 8

    def chip_on(steps):
        return lax.rem(me + 2 * steps + count, count)

    def rows(owner, offset, size):
        return pl.ds(pl.multiple_of(owner * quarter + offset, eighth), size)

    far_to = lax.rem(me + 7, count)
    far_from = lax.rem(me - 7 + count, count)
    barrier = pltpu.get_barrier_semaphore()
    for steps in (1, 2, 3):
        pl.semaphore_signal(
            barrier, inc=1, device_id={"sp": chip_on(-steps), "tp": col}, device_id_type=MESH
        )
    for to in (east, west):
        pl.semaphore_signal(barrier, inc=1, device_id={"sp": me, "tp": to}, device_id_type=MESH)
    pl.semaphore_signal(
        barrier, inc=1, device_id={"sp": sibling, "tp": col}, device_id_type=MESH
    )

    @pl.when(core == 0)
    def _():
        pl.semaphore_signal(
            barrier, inc=1, device_id={"sp": far_from, "tp": col}, device_id_type=MESH
        )
        pl.semaphore_wait(barrier, 6)

    @pl.when(core == 1)
    def _():
        pl.semaphore_wait(barrier, 7)

    def y_copy(steps):
        part = rows(col, 0, quarter)
        return copy_to(
            pay_ref.at[part],
            win_ref.at[2 * steps, part],
            y_send.at[steps],
            y_recv.at[steps],
            chip_on(steps),
            col,
        )

    def far_copy():
        part = rows(col, 0, quarter)
        return copy_to(
            pay_ref.at[part], win_ref.at[7, part], y_send.at[4], y_recv.at[4], far_to, col
        )

    def x_copy(lane, slot, kind):
        if kind == 0:
            part, to = rows(col, 0, quarter), east
        elif kind == 1:
            part, to = rows(col, 0, quarter), west
        elif kind == 2:
            part, to = rows(west, 0, eighth), east
        else:
            part, to = rows(east, eighth, eighth), west
        return copy_to(
            win_ref.at[slot, part],
            win_ref.at[slot, part],
            x_send.at[lane, kind],
            x_recv.at[lane, kind],
            me,
            to,
        )

    def d_copy(index, src, slot):
        return copy_to(
            src, win_ref.at[slot], d_send.at[index], d_recv.at[index], sibling, col
        )

    own = pltpu.make_async_copy(pay_ref, win_ref.at[0], own_sem)
    own.start()
    for steps in (1, 2, 3):
        y_copy(steps).start()

    @pl.when(core == 1)
    def _():
        far_copy().start()

    @pl.when(core == 0)
    def _():
        d_copy(0, pay_ref, 1).start()

    def spread(lane, slot):
        x_copy(lane, slot, 0).start()
        x_copy(lane, slot, 1).start()

    def relay(lane, slot):
        x_copy(lane, slot, 0).wait_recv()
        x_copy(lane, slot, 2).start()
        x_copy(lane, slot, 1).wait_recv()
        x_copy(lane, slot, 3).start()

    def finish(lane, slot):
        x_copy(lane, slot, 2).wait_recv()
        x_copy(lane, slot, 3).wait_recv()

    def to_sibling(steps):
        @pl.when(core == 0)
        def _():
            d_copy(steps, win_ref.at[2 * steps], 2 * steps + 1).start()

        @pl.when(core == 1)
        def _():
            d_copy(steps, win_ref.at[2 * steps], 2 * steps - 1).start()

    y_copy(1).wait_recv()
    spread(1, 2)
    y_copy(2).wait_recv()
    spread(2, 4)
    relay(1, 2)
    y_copy(3).wait_recv()
    spread(3, 6)
    finish(1, 2)
    to_sibling(1)
    relay(2, 4)

    @pl.when(core == 0)
    def _():
        far_copy().wait_recv()
        spread(4, 7)

    finish(2, 4)
    to_sibling(2)
    relay(3, 6)

    @pl.when(core == 0)
    def _():
        relay(4, 7)

    finish(3, 6)
    to_sibling(3)

    @pl.when(core == 0)
    def _():
        finish(4, 7)

    own.wait()
    for steps in (1, 2, 3):
        y_copy(steps).wait_send()
        for kind in range(4):
            x_copy(steps, 2 * steps, kind).wait_send()

    @pl.when(core == 0)
    def _():
        d_copy(0, pay_ref, 1).wait_send()
        for steps in (1, 2, 3):
            d_copy(steps, win_ref.at[2 * steps], 2 * steps + 1).wait_send()
            d_copy(steps, win_ref.at[2 * steps], 2 * steps - 1).wait_recv()
        for kind in range(4):
            x_copy(4, 7, kind).wait_send()

    @pl.when(core == 1)
    def _():
        far_copy().wait_send()
        d_copy(0, pay_ref, 1).wait_recv()
        for steps in (1, 2, 3):
            d_copy(steps, win_ref.at[2 * steps], 2 * steps - 1).wait_send()
            d_copy(steps, win_ref.at[2 * steps], 2 * steps + 1).wait_recv()


def attention_kernel(
    latent_ref,
    start_ref,
    win_ref,
    cos_ref,
    sin_ref,
    gain_ref,
    content_ref,
    rotary_ref,
    key_ref,
    value_ref,
    out_ref,
    query,
    highest,
    denominator,
    summed,
):
    length, rank = latent_ref.shape[0], key_ref.shape[0]
    heads = key_ref.shape[1] // CONTENT
    anchor = lax.axis_index("sp") * length
    scale = (CONTENT + ROTARY) ** (-0.5) * LOG2E
    normed = rms_scale(latent_ref[...], gain_ref[...])
    content = jnp.dot(normed, content_ref[...], preferred_element_type=F32).astype(BF16)
    raw = jnp.dot(normed, rotary_ref[...], preferred_element_type=F32)
    lane = lax.broadcasted_iota(jnp.int32, (length, 2 * ROTARY), 1)
    for head in range(heads):
        pair = raw[:, (head // 2) * 2 * ROTARY : (head // 2 + 1) * 2 * ROTARY]
        turned = rotate(pair, cos_ref[...], sin_ref[...])
        turned = jnp.where(lane // ROTARY == head % 2, turned, 0.0).astype(BF16)
        query[head, :, :CONTENT] = content[:, head * CONTENT : (head + 1) * CONTENT]
        query[head, :, CONTENT:] = turned
    highest[...] = jnp.full(highest.shape, MASKED, F32)
    denominator[...] = jnp.zeros(denominator.shape, F32)
    summed[...] = jnp.zeros(summed.shape, F32)
    starts = start_ref[...]
    places = anchor + lax.broadcasted_iota(jnp.int32, (length, 1), 0)

    def absorb(slot, carry):
        shared = win_ref[slot, :, :rank]
        turn = win_ref[slot, :, rank:]
        keys = jnp.dot(shared, key_ref[...], preferred_element_type=F32).astype(BF16)
        values = jnp.dot(shared, value_ref[...], preferred_element_type=F32).astype(BF16)
        key_places = (
            anchor - slot * length + lax.broadcasted_iota(jnp.int32, (length, length), 1)
        )
        visible = (key_places >= starts) & (key_places <= places)
        for head in range(heads):
            cut = slice(head * CONTENT, (head + 1) * CONTENT)
            joined = jnp.concatenate([keys[:, cut], turn], axis=1)
            scores = lax.dot_general(
                query[head], joined, (((1,), (1,)), ((), ())), preferred_element_type=F32
            )
            scores = jnp.where(visible, scores * scale, MASKED)
            before = highest[head]
            after = jnp.maximum(before, jnp.max(scores, axis=-1, keepdims=True))
            factor = jnp.exp2(before - after)
            weights = jnp.exp2(scores - after)
            highest[head] = after
            denominator[head] = denominator[head] * factor + jnp.sum(
                weights, axis=-1, keepdims=True
            )
            summed[head] = summed[head] * factor + jnp.dot(
                weights.astype(BF16), values[:, cut], preferred_element_type=F32
            )
        return carry

    lax.fori_loop(0, SPAN, absorb, 0)
    for head in range(heads):
        cut = slice(head * CONTENT, (head + 1) * CONTENT)
        out_ref[:, cut] = (summed[head] / denominator[head]).astype(BF16)


CHUNKS = 4


def output_kernel(
    attended_ref, weight_ref, out_ref, term, first, second, held, sums, send, recv
):
    col = lax.axis_index("tp")
    me = lax.axis_index("sp")
    ring = lax.axis_size("tp")
    length, model = out_ref.shape
    size = length // CHUNKS
    half, piece = model // 4, model // 8
    bit = col // 2
    gray = lax.rem(col + bit, 2)
    near = (col + 1 - 2 * lax.rem(col, 2), ring - 1 - col)
    keep = (gray, bit)
    sub = (bit, gray)

    barrier = pltpu.get_barrier_semaphore()
    for partner in near:
        pl.semaphore_signal(
            barrier, inc=1, device_id={"sp": me, "tp": partner}, device_id_type=MESH
        )
    pl.semaphore_wait(barrier, 2)

    def rows(chunk):
        return pl.ds(chunk * size, size)

    def half_at(side, which):
        return pl.multiple_of(side * (model // 2) + which * half, half)

    def piece_at(side, which, sub_which):
        return pl.multiple_of(side * (model // 2) + which * half + sub_which * piece, piece)

    def copy(kind, side, chunk, src, dst, partner):
        return copy_to(
            src, dst, send.at[kind, side, chunk], recv.at[kind, side, chunk], me, partner
        )

    def stage_one(side, chunk):
        return copy(
            0,
            side,
            chunk,
            term.at[rows(chunk), pl.ds(half_at(side, 1 - keep[side]), half)],
            first.at[side, rows(chunk)],
            near[side],
        )

    def stage_two(side, chunk):
        return copy(
            1,
            side,
            chunk,
            held.at[side, rows(chunk)],
            second.at[side, rows(chunk)],
            near[1 - side],
        )

    def own_piece(side, chunk):
        return out_ref.at[rows(chunk), pl.ds(piece_at(side, keep[side], sub[side]), piece)]

    def gather(kind, side, chunk):
        if kind == 4:
            ref = out_ref.at[
                rows(chunk), pl.ds(piece_at(side, keep[side], 1 - sub[side]), piece)
            ]
        else:
            ref = own_piece(side, chunk)
        return copy(kind, side, chunk, ref, ref, near[1 - side] if kind == 2 else near[side])

    for chunk in range(CHUNKS):
        mine = attended_ref[rows(chunk), :]
        for block in range(model // half):
            cut = pl.ds(block * half, half)
            term[rows(chunk), cut] = jnp.dot(
                mine, weight_ref[:, cut], preferred_element_type=F32
            ).astype(BF16)
        for side in (0, 1):
            stage_one(side, chunk).start()

    for chunk in range(CHUNKS):
        for side in (0, 1):
            stage_one(side, chunk).wait_recv()
            base = half_at(side, keep[side])
            theirs = pl.multiple_of((1 - sub[side]) * piece, piece)
            ours = pl.multiple_of(sub[side] * piece, piece)
            held[side, rows(chunk), :] = (
                term[rows(chunk), pl.ds(pl.multiple_of(base + theirs, piece), piece)].astype(F32)
                + first[side, rows(chunk), pl.ds(theirs, piece)].astype(F32)
            ).astype(BF16)
            stage_two(side, chunk).start()
            sums[side, rows(chunk), :] = term[
                rows(chunk), pl.ds(pl.multiple_of(base + ours, piece), piece)
            ].astype(F32) + first[side, rows(chunk), pl.ds(ours, piece)].astype(F32)

    for chunk in range(CHUNKS):
        for side in (0, 1):
            stage_two(side, chunk).wait_recv()
            cut = pl.ds(piece_at(side, keep[side], sub[side]), piece)
            out_ref[rows(chunk), cut] = (
                sums[side, rows(chunk), :] + second[side, rows(chunk), :].astype(F32)
            ).astype(BF16)
            gather(2, side, chunk).start()
            gather(3, side, chunk).start()

    for chunk in range(CHUNKS):
        for side in (0, 1):
            gather(2, side, chunk).wait_recv()
            gather(4, side, chunk).start()

    for chunk in range(CHUNKS):
        for side in (0, 1):
            gather(3, side, chunk).wait_recv()
            gather(4, side, chunk).wait_recv()
            stage_one(side, chunk).wait_send()
            stage_two(side, chunk).wait_send()
            for kind in (2, 3, 4):
                gather(kind, side, chunk).wait_send()


def on_device(
    query_latent,
    shared_latent,
    rotary_key,
    document_start,
    query_gain,
    shared_gain,
    content_weight,
    rotary_weight,
    key_weight,
    value_weight,
    output_weight,
):
    length = query_latent.shape[0]
    rank = shared_latent.shape[1]
    model = output_weight.shape[1]
    heads = key_weight.shape[1] // CONTENT
    width = rank + 2 * ROTARY
    places = lax.axis_index("sp") * length + jnp.arange(length, dtype=jnp.int32)
    frequency = 1.0 / THETA ** (jnp.arange(0, ROTARY, 2, dtype=F32) / ROTARY)
    angles = places.astype(F32)[:, None] * frequency[None, :]
    cosine, sine = jnp.cos(angles), jnp.sin(angles)
    cosine = jnp.concatenate([cosine] * 4, axis=1)
    sine = jnp.concatenate([-sine, sine, -sine, sine], axis=1)
    rotary_pair = jnp.concatenate([rotary_key, rotary_key], axis=1)
    payload = pl.pallas_call(
        payload_kernel,
        out_shape=jax.ShapeDtypeStruct((length, width), BF16),
        in_specs=[WHOLE] * 5,
        out_specs=WHOLE,
        name="payload",
    )(shared_latent, rotary_pair, cosine, sine, shared_gain[None, :])
    window = pl.pallas_call(
        exchange_kernel,
        out_shape=jax.ShapeDtypeStruct((SPAN, length, width), BF16),
        in_specs=[WHOLE],
        out_specs=WHOLE,
        scratch_shapes=[
            pltpu.SemaphoreType.DMA,
            pltpu.SemaphoreType.DMA((5,)),
            pltpu.SemaphoreType.DMA((5,)),
            pltpu.SemaphoreType.DMA((5, 4)),
            pltpu.SemaphoreType.DMA((5, 4)),
            pltpu.SemaphoreType.DMA((4,)),
            pltpu.SemaphoreType.DMA((4,)),
        ],
        compiler_params=pltpu.CompilerParams(collective_id=0, has_side_effects=True),
        name="exchange",
    )(payload)
    attended = pl.pallas_call(
        attention_kernel,
        out_shape=jax.ShapeDtypeStruct((length, heads * CONTENT), BF16),
        in_specs=[WHOLE] * 10,
        out_specs=WHOLE,
        scratch_shapes=[
            pltpu.VMEM((heads, length, 2 * CONTENT), BF16),
            pltpu.VMEM((heads, length, 1), F32),
            pltpu.VMEM((heads, length, 1), F32),
            pltpu.VMEM((heads, length, CONTENT), F32),
        ],
        name="attention",
    )(
        query_latent,
        document_start[:, None],
        window,
        cosine,
        sine,
        query_gain[None, :],
        content_weight,
        rotary_weight,
        key_weight,
        value_weight,
    )
    mixed = pl.pallas_call(
        output_kernel,
        out_shape=jax.ShapeDtypeStruct((length, model), BF16),
        in_specs=[WHOLE] * 2,
        out_specs=WHOLE,
        scratch_shapes=[
            pltpu.VMEM((length, model), BF16),
            pltpu.VMEM((2, length, model // 4), BF16),
            pltpu.VMEM((2, length, model // 8), BF16),
            pltpu.VMEM((2, length, model // 8), BF16),
            pltpu.VMEM((2, length, model // 8), F32),
            pltpu.SemaphoreType.DMA((5, 2, CHUNKS)),
            pltpu.SemaphoreType.DMA((5, 2, CHUNKS)),
        ],
        compiler_params=pltpu.CompilerParams(collective_id=1, has_side_effects=True),
        name="output",
    )(attended, output_weight)
    return mixed


def solution(mesh):
    return jax.shard_map(
        on_device,
        mesh=mesh,
        in_specs=(
            P("sp", None),
            P("sp", None),
            P("sp", None),
            P("sp"),
            P(),
            P(),
            P(None, "tp"),
            P(None, "tp"),
            P(None, "tp"),
            P(None, "tp"),
            P("tp", None),
        ),
        out_specs=P("sp", None),
        check_vma=False,
    )
```

```python
import jax
import jax.numpy as jnp
from jax import lax
from jax.experimental import pallas as pl
from jax.experimental.pallas import tpu as pltpu
from jax.sharding import PartitionSpec as P

MESH = pl.DeviceIdType.MESH
CONTENT = 128
ROTARY = 64
SPAN = 8
NORM_EPS = 1e-06
THETA = 10000.0
MASKED = -1e30
LOG2E = 1.4426950408889634
F32 = jnp.float32
BF16 = jnp.bfloat16
WHOLE = pl.BlockSpec(memory_space=pltpu.VMEM)
FAR = pl.BlockSpec(memory_space=pltpu.HBM)
CHUNKS = 4


def copy_to(src, dst, send, recv, sp, tp):
    return pltpu.make_async_remote_copy(
        src_ref=src,
        dst_ref=dst,
        send_sem=send,
        recv_sem=recv,
        device_id={"sp": sp, "tp": tp},
        device_id_type=MESH,
    )


def rms_scale(entries, gain):
    entries = entries.astype(F32)
    mean = jnp.mean(entries * entries, axis=-1, keepdims=True)
    return (entries * lax.rsqrt(mean + NORM_EPS) * gain).astype(BF16)


def rotate(entries, cosine, sine):
    width = entries.shape[-1]
    lane = lax.broadcasted_iota(jnp.int32, entries.shape, 1)
    ahead = pltpu.roll(entries, width - ROTARY // 2, 1)
    behind = pltpu.roll(entries, ROTARY // 2, 1)
    other = jnp.where(lane % ROTARY < ROTARY // 2, ahead, behind)
    return entries * cosine + other * sine


def mixed_kernel(
    latent_hbm,
    shared_ref,
    rotary_ref,
    start_ref,
    cos_ref,
    sin_ref,
    query_gain_ref,
    shared_gain_ref,
    content_hbm,
    rotary_weight_hbm,
    key_hbm,
    value_hbm,
    output_hbm,
    out_ref,
    latent_ref,
    content_ref,
    rotary_weight_ref,
    key_ref,
    value_ref,
    weight_ref,
    value_turned,
    pay_ref,
    win_ref,
    query,
    highest,
    denominator,
    summed,
    attended,
    term,
    first,
    second,
    held,
    load_sem,
    y_send,
    y_recv,
    x_send,
    x_recv,
    d_send,
    d_recv,
    send,
    recv,
):
    count, ring = lax.axis_size("sp"), lax.axis_size("tp")
    me, col = lax.axis_index("sp"), lax.axis_index("tp")
    core = lax.rem(me, 2)
    chip, chips = me // 2, count // 2
    sibling = me + 1 - 2 * core
    east, west = lax.rem(col + 1, ring), lax.rem(col + ring - 1, ring)
    length, rank = shared_ref.shape
    heads = key_ref.shape[1] // CONTENT
    model = out_ref.shape[1]
    quarter, eighth = length // 4, length // 8

    def load(index, src, dst):
        return pltpu.make_async_copy(src, dst, load_sem.at[index])

    loads = [
        load(0, latent_hbm, latent_ref),
        load(1, content_hbm, content_ref),
        load(2, rotary_weight_hbm, rotary_weight_ref),
        load(3, value_hbm, value_ref),
        load(4, key_hbm, key_ref),
        load(5, output_hbm, weight_ref),
    ]
    for item in loads:
        item.start()

    barrier = pltpu.get_barrier_semaphore()

    def greet(sp, tp):
        pl.semaphore_signal(barrier, inc=1, device_id={"sp": sp, "tp": tp}, device_id_type=MESH)

    def has(steps):
        return chip >= steps

    def feeds(steps):
        return chip + steps < chips

    greet(me, east)
    greet(me, west)
    greet(sibling, col)
    for steps in (1, 2, 3):

        @pl.when(has(steps))
        def _():
            greet(me - 2 * steps, col)

    @pl.when((core == 0) & has(4))
    def _():
        greet(me - 7, col)

    pay_ref[:, :rank] = rms_scale(shared_ref[...], shared_gain_ref[...])
    leading = rotary_ref[: ROTARY // 2, :].astype(F32)
    trailing = rotary_ref[ROTARY // 2 :, :].astype(F32)
    cosine, sine = cos_ref[...], sin_ref[...]
    turned = [leading * cosine - trailing * sine, leading * sine + trailing * cosine]
    pay_ref[:, rank:] = jnp.concatenate(turned * 2, axis=0).T.astype(BF16)

    def rows(owner, offset, size):
        return pl.ds(pl.multiple_of(owner * quarter + offset, eighth), size)

    def y_copy(steps):
        part = rows(col, 0, quarter)
        slot, to = (2 * steps, me + 2 * steps) if steps < 4 else (7, me + 7)
        return copy_to(
            pay_ref.at[part], win_ref.at[slot, part], y_send.at[steps], y_recv.at[steps], to, col
        )

    def x_copy(lane, kind):
        slot = 2 * lane if lane < 4 else 7
        if kind == 0:
            part, to = rows(col, 0, quarter), east
        elif kind == 1:
            part, to = rows(col, 0, quarter), west
        elif kind == 2:
            part, to = rows(west, 0, eighth), east
        else:
            part, to = rows(east, eighth, eighth), west
        ref = win_ref.at[slot, part]
        return copy_to(ref, ref, x_send.at[lane, kind], x_recv.at[lane, kind], me, to)

    def d_copy(lane, shift):
        src = win_ref.at[2 * lane] if lane else pay_ref
        return copy_to(
            src, win_ref.at[2 * lane + shift], d_send.at[lane], d_recv.at[lane], sibling, col
        )

    def on_core(which, also=None):
        mine = core == which
        return pl.when(mine if also is None else mine & also)

    far = (core == 1) & feeds(4)
    number = 3 + jnp.minimum(3, chips - 1 - chip) + far.astype(jnp.int32)
    pl.semaphore_wait(barrier, number)
    for steps in (1, 2, 3):

        @pl.when(feeds(steps))
        def _():
            y_copy(steps).start()

    @pl.when(far)
    def _():
        y_copy(4).start()

    @on_core(0)
    def _():
        d_copy(0, 1).start()

    def arrived(lane):
        y_copy(lane).wait_recv()
        x_copy(lane, 0).start()
        x_copy(lane, 1).start()

    def relay(lane):
        x_copy(lane, 0).wait_recv()
        x_copy(lane, 2).start()
        x_copy(lane, 1).wait_recv()
        x_copy(lane, 3).start()

    def finish(lane):
        x_copy(lane, 2).wait_recv()
        x_copy(lane, 3).wait_recv()
        if lane < 4:

            @on_core(0)
            def _():
                d_copy(lane, 1).start()

            @on_core(1)
            def _():
                d_copy(lane, -1).start()

    def from_sibling(lane):
        @on_core(0)
        def _():
            d_copy(lane, -1).wait_recv()

        @on_core(1)
        def _():
            d_copy(lane, 1).wait_recv()

    scale = (CONTENT + ROTARY) ** (-0.5) * LOG2E
    for item in loads[:3]:
        item.wait()
    normed = rms_scale(latent_ref[...], query_gain_ref[...])
    content = jnp.dot(normed, content_ref[...], preferred_element_type=F32).astype(BF16)
    raw = jnp.dot(normed, rotary_weight_ref[...], preferred_element_type=F32)
    wide_cosine = jnp.concatenate([cosine] * 4, axis=0).T
    wide_sine = jnp.concatenate([-sine, sine, -sine, sine], axis=0).T
    lane_of = lax.broadcasted_iota(jnp.int32, (length, 2 * ROTARY), 1)
    for head in range(heads):
        cut = slice(head // 2 * 2 * ROTARY, (head // 2 + 1) * 2 * ROTARY)
        pair = rotate(raw[:, cut], wide_cosine, wide_sine)
        pair = jnp.where(lane_of // ROTARY == head % 2, pair, 0.0).astype(BF16)
        query[head, :, :CONTENT] = content[:, head * CONTENT : (head + 1) * CONTENT]
        query[head, :, CONTENT:] = pair
    highest[...] = jnp.full(highest.shape, MASKED, F32)
    denominator[...] = jnp.zeros(denominator.shape, F32)
    summed[...] = jnp.zeros(summed.shape, F32)
    loads[3].wait()
    value_turned[...] = value_ref[...].astype(F32).T.astype(BF16)
    loads[4].wait()
    anchor = me * length

    def absorb(slot, block_ref):
        shared = block_ref[:, :rank]
        turn = block_ref[:, rank:]
        keys = jnp.dot(shared, key_ref[...], preferred_element_type=F32).astype(BF16)
        values = lax.dot_general(
            value_turned[...], shared, (((1,), (1,)), ((), ())), preferred_element_type=F32
        ).astype(BF16)
        shape = (length, length)
        key_places = anchor - slot * length + lax.broadcasted_iota(jnp.int32, shape, 0)
        visible = key_places >= start_ref[...]
        if isinstance(slot, int) and slot == 0:
            visible = visible & (
                lax.broadcasted_iota(jnp.int32, shape, 0)
                <= lax.broadcasted_iota(jnp.int32, shape, 1)
            )
        for head in range(heads):
            cut = slice(head * CONTENT, (head + 1) * CONTENT)
            joined = jnp.concatenate([keys[:, cut], turn], axis=1)
            scores = lax.dot_general(
                joined, query[head], (((1,), (1,)), ((), ())), preferred_element_type=F32
            )
            scores = jnp.where(visible, scores * scale, MASKED)
            before = highest[head]
            after = jnp.maximum(before, jnp.max(scores, axis=0, keepdims=True))
            factor = jnp.exp2(before - after)
            weights = jnp.exp2(scores - after)
            highest[head] = after
            denominator[head] = denominator[head] * factor + jnp.sum(
                weights, axis=0, keepdims=True
            )
            summed[head] = summed[head] * factor + jnp.dot(
                values[cut, :], weights.astype(BF16), preferred_element_type=F32
            )

    def absorb_slot(slot):
        absorb(slot, win_ref.at[slot])

    absorb(0, pay_ref)

    @on_core(1)
    def _():
        d_copy(0, 1).wait_recv()
        absorb_slot(1)

    def absorb_sibling(lane):
        from_sibling(lane)
        absorb_slot(2 * lane - 1 + 2 * core)

    @pl.when(has(1))
    def _():
        arrived(1)
        relay(1)

    @pl.when(has(2))
    def _():
        arrived(2)

    @pl.when(has(1))
    def _():
        finish(1)
        absorb_slot(2)

    @pl.when(has(2))
    def _():
        relay(2)

    @pl.when(has(1))
    def _():
        absorb_sibling(1)

    @pl.when(has(2))
    def _():
        finish(2)

    @pl.when(has(3))
    def _():
        arrived(3)

    @on_core(0, has(4))
    def _():
        arrived(4)

    @pl.when(has(2))
    def _():
        absorb_slot(4)

    @pl.when(has(3))
    def _():
        relay(3)

    @on_core(0, has(4))
    def _():
        relay(4)

    @pl.when(has(2))
    def _():
        absorb_sibling(2)

    @pl.when(has(3))
    def _():
        finish(3)
        absorb_slot(6)
        absorb_sibling(3)

    @on_core(0, has(4))
    def _():
        finish(4)
        absorb_slot(7)

    for head in range(heads):
        cut = slice(head * CONTENT, (head + 1) * CONTENT)
        attended[:, cut] = (summed[head] / denominator[head]).T.astype(BF16)
    loads[5].wait()

    size = length // CHUNKS
    half, piece = model // 4, model // 8
    bit = col // 2
    gray = lax.rem(col + bit, 2)
    near = (col + 1 - 2 * lax.rem(col, 2), ring - 1 - col)
    keep = (gray, bit)
    sub = (bit, gray)

    def part(chunk):
        return pl.ds(chunk * size, size)

    def half_at(side, which):
        return pl.multiple_of(side * (model // 2) + which * half, half)

    def piece_at(side, which, sub_which):
        return pl.multiple_of(side * (model // 2) + which * half + sub_which * piece, piece)

    def copy(kind, side, chunk, src, dst, partner):
        return copy_to(
            src, dst, send.at[kind, side, chunk], recv.at[kind, side, chunk], me, partner
        )

    def stage_one(side, chunk):
        return copy(
            0, side, chunk, term.at[side, part(chunk)], first.at[side, part(chunk)], near[side]
        )

    def stage_two(side, chunk):
        return copy(
            1, side, chunk, held.at[side, part(chunk)], second.at[side, part(chunk)], near[1 - side]
        )

    def gather(kind, side, chunk):
        which = 1 - sub[side] if kind == 4 else sub[side]
        ref = out_ref.at[part(chunk), pl.ds(piece_at(side, keep[side], which), piece)]
        return copy(kind, side, chunk, ref, ref, near[1 - side] if kind == 2 else near[side])

    def project(chunk, at, width):
        return jnp.dot(
            attended[part(chunk), :], weight_ref[:, pl.ds(at, width)], preferred_element_type=F32
        ).astype(BF16)

    for chunk in range(CHUNKS):
        for side in (0, 1):
            term[side, part(chunk), :] = project(chunk, half_at(side, 1 - keep[side]), half)
            stage_one(side, chunk).start()

    for chunk in range(CHUNKS):
        for side in (0, 1):
            theirs = pl.multiple_of((1 - sub[side]) * piece, piece)
            mine = project(chunk, piece_at(side, keep[side], 1 - sub[side]), piece)
            stage_one(side, chunk).wait_recv()
            held[side, part(chunk), :] = (
                mine.astype(F32) + first[side, part(chunk), pl.ds(theirs, piece)].astype(F32)
            ).astype(BF16)
            stage_two(side, chunk).start()

    for chunk in range(CHUNKS):
        for side in (0, 1):
            ours = pl.multiple_of(sub[side] * piece, piece)
            at = piece_at(side, keep[side], sub[side])
            mine = project(chunk, at, piece).astype(F32)
            mine = mine + first[side, part(chunk), pl.ds(ours, piece)].astype(F32)
            stage_two(side, chunk).wait_recv()
            out_ref[part(chunk), pl.ds(at, piece)] = (
                mine + second[side, part(chunk), :].astype(F32)
            ).astype(BF16)
            gather(2, side, chunk).start()
            gather(3, side, chunk).start()

    for chunk in range(CHUNKS):
        for side in (0, 1):
            gather(2, side, chunk).wait_recv()
            gather(4, side, chunk).start()

    for chunk in range(CHUNKS):
        for side in (0, 1):
            gather(3, side, chunk).wait_recv()
            gather(4, side, chunk).wait_recv()
            stage_one(side, chunk).wait_send()
            stage_two(side, chunk).wait_send()
            for kind in (2, 3, 4):
                gather(kind, side, chunk).wait_send()

    for steps in (1, 2, 3):

        @pl.when(feeds(steps))
        def _():
            y_copy(steps).wait_send()

        @pl.when(has(steps))
        def _():
            for kind in range(4):
                x_copy(steps, kind).wait_send()
            d_copy(steps, -1).wait_send()

    @pl.when(far)
    def _():
        y_copy(4).wait_send()

    @on_core(0)
    def _():
        d_copy(0, 1).wait_send()

    @on_core(0, has(4))
    def _():
        for kind in range(4):
            x_copy(4, kind).wait_send()


def on_device(
    query_latent,
    shared_latent,
    rotary_key,
    document_start,
    query_gain,
    shared_gain,
    content_weight,
    rotary_weight,
    key_weight,
    value_weight,
    output_weight,
):
    length, query_rank = query_latent.shape
    rank = shared_latent.shape[1]
    model = output_weight.shape[1]
    heads = key_weight.shape[1] // CONTENT
    width = rank + 2 * ROTARY
    places = lax.axis_index("sp") * length + jnp.arange(length, dtype=jnp.int32)
    frequency = 1.0 / THETA ** (jnp.arange(0, ROTARY, 2, dtype=F32) / ROTARY)
    angles = frequency[:, None] * places.astype(F32)[None, :]
    vmem, dma = pltpu.VMEM, pltpu.SemaphoreType.DMA
    return pl.pallas_call(
        mixed_kernel,
        out_shape=jax.ShapeDtypeStruct((length, model), BF16),
        in_specs=[FAR] + [WHOLE] * 7 + [FAR] * 5,
        out_specs=WHOLE,
        scratch_shapes=[
            vmem((length, query_rank), BF16),
            vmem(content_weight.shape, BF16),
            vmem(rotary_weight.shape, BF16),
            vmem(key_weight.shape, BF16),
            vmem(value_weight.shape, BF16),
            vmem(output_weight.shape, BF16),
            vmem(value_weight.shape[::-1], BF16),
            vmem((length, width), BF16),
            vmem((SPAN, length, width), BF16),
            vmem((heads, length, 2 * CONTENT), BF16),
            vmem((heads, 1, length), F32),
            vmem((heads, 1, length), F32),
            vmem((heads, CONTENT, length), F32),
            vmem((length, heads * CONTENT), BF16),
            vmem((2, length, model // 4), BF16),
            vmem((2, length, model // 4), BF16),
            vmem((2, length, model // 8), BF16),
            vmem((2, length, model // 8), BF16),
            dma((6,)),
            dma((5,)),
            dma((5,)),
            dma((5, 4)),
            dma((5, 4)),
            dma((4,)),
            dma((4,)),
            dma((5, 2, CHUNKS)),
            dma((5, 2, CHUNKS)),
        ],
        compiler_params=pltpu.CompilerParams(
            collective_id=0, has_side_effects=True, vmem_limit_bytes=46 * 2**20
        ),
        name="mixed",
    )(
        query_latent,
        shared_latent,
        rotary_key.T,
        document_start[None, :],
        jnp.cos(angles),
        jnp.sin(angles),
        query_gain[None, :],
        shared_gain[None, :],
        content_weight,
        rotary_weight,
        key_weight,
        value_weight,
        output_weight,
    )


def solution(mesh):
    return jax.shard_map(
        on_device,
        mesh=mesh,
        in_specs=(
            P("sp", None),
            P("sp", None),
            P("sp", None),
            P("sp"),
            P(),
            P(),
            P(None, "tp"),
            P(None, "tp"),
            P(None, "tp"),
            P(None, "tp"),
            P("tp", None),
        ),
        out_specs=P("sp", None),
        check_vma=False,
    )
```

```python
import jax
import jax.numpy as jnp
from jax import lax
from jax.experimental import pallas as pl
from jax.experimental.pallas import tpu as pltpu
from jax.sharding import PartitionSpec as P

MESH = pl.DeviceIdType.MESH
CONTENT = 128
ROTARY = 64
SPAN = 8
NORM_EPS = 1e-06
THETA = 10000.0
MASKED = -1e30
LOG2E = 1.4426950408889634
F32 = jnp.float32
BF16 = jnp.bfloat16
WHOLE = pl.BlockSpec(memory_space=pltpu.VMEM)
FAR = pl.BlockSpec(memory_space=pltpu.HBM)
CHUNKS = 4


def copy_to(src, dst, send, recv, sp, tp):
    return pltpu.make_async_remote_copy(
        src_ref=src,
        dst_ref=dst,
        send_sem=send,
        recv_sem=recv,
        device_id={"sp": sp, "tp": tp},
        device_id_type=MESH,
    )


def rms_scale(entries, gain):
    entries = entries.astype(F32)
    mean = jnp.mean(entries * entries, axis=-1, keepdims=True)
    return (entries * lax.rsqrt(mean + NORM_EPS) * gain).astype(BF16)


def rotate(entries, cosine, sine):
    width = entries.shape[-1]
    lane = lax.broadcasted_iota(jnp.int32, entries.shape, 1)
    ahead = pltpu.roll(entries, width - ROTARY // 2, 1)
    behind = pltpu.roll(entries, ROTARY // 2, 1)
    other = jnp.where(lane % ROTARY < ROTARY // 2, ahead, behind)
    return entries * cosine + other * sine


def mixed_kernel(
    latent_hbm,
    shared_ref,
    rotary_ref,
    start_ref,
    cos_ref,
    sin_ref,
    query_gain_ref,
    shared_gain_ref,
    content_hbm,
    rotary_weight_hbm,
    key_hbm,
    value_hbm,
    output_hbm,
    out_ref,
    latent_ref,
    content_ref,
    rotary_weight_ref,
    key_ref,
    value_ref,
    weight_ref,
    value_turned,
    pay_ref,
    win_ref,
    query,
    highest,
    denominator,
    summed,
    attended,
    term,
    first,
    second,
    held,
    load_sem,
    y_send,
    y_recv,
    x_send,
    x_recv,
    d_send,
    d_recv,
    send,
    recv,
):
    count, ring = lax.axis_size("sp"), lax.axis_size("tp")
    me, col = lax.axis_index("sp"), lax.axis_index("tp")
    core = lax.rem(me, 2)
    chip, chips = me // 2, count // 2
    sibling = me + 1 - 2 * core
    east, west = lax.rem(col + 1, ring), lax.rem(col + ring - 1, ring)
    length, rank = shared_ref.shape
    heads = key_ref.shape[1] // CONTENT
    model = out_ref.shape[1]
    quarter, eighth = length // 4, length // 8

    def load(index, src, dst):
        return pltpu.make_async_copy(src, dst, load_sem.at[index])

    loads = [
        load(0, latent_hbm, latent_ref),
        load(1, content_hbm, content_ref),
        load(2, rotary_weight_hbm, rotary_weight_ref),
        load(3, value_hbm, value_ref),
        load(4, key_hbm, key_ref),
        load(5, output_hbm, weight_ref),
    ]
    for item in loads:
        item.start()

    barrier = pltpu.get_barrier_semaphore()

    def greet(sp, tp):
        pl.semaphore_signal(barrier, inc=1, device_id={"sp": sp, "tp": tp}, device_id_type=MESH)

    def has(steps):
        return chip >= steps

    def feeds(steps):
        return chip + steps < chips

    greet(me, east)
    greet(me, west)
    greet(sibling, col)
    for steps in (1, 2):

        @pl.when(has(steps))
        def _():
            greet(me - 2 * steps, col)

    @pl.when((core == 0) & has(4))
    def _():
        greet(me - 3, col)

    pay_ref[:, :rank] = rms_scale(shared_ref[...], shared_gain_ref[...])
    leading = rotary_ref[: ROTARY // 2, :].astype(F32)
    trailing = rotary_ref[ROTARY // 2 :, :].astype(F32)
    cosine, sine = cos_ref[...], sin_ref[...]
    turned = [leading * cosine - trailing * sine, leading * sine + trailing * cosine]
    pay_ref[:, rank:] = jnp.concatenate(turned * 2, axis=0).T.astype(BF16)

    def rows(owner, offset, size):
        return pl.ds(pl.multiple_of(owner * quarter + offset, eighth), size)

    def y_copy(steps):
        part = rows(col, 0, quarter)
        src = pay_ref.at[part] if steps < 3 else win_ref.at[4, part]
        slot, to = ((2, me + 2), (4, me + 4), (6, me + 2), (7, me + 3))[steps - 1]
        return copy_to(
            src, win_ref.at[slot, part], y_send.at[steps], y_recv.at[steps], to, col
        )

    def x_copy(lane, kind):
        slot = 2 * lane if lane < 4 else 7
        if kind == 0:
            part, to = rows(col, 0, quarter), east
        elif kind == 1:
            part, to = rows(col, 0, quarter), west
        elif kind == 2:
            part, to = rows(west, 0, eighth), east
        else:
            part, to = rows(east, eighth, eighth), west
        ref = win_ref.at[slot, part]
        return copy_to(ref, ref, x_send.at[lane, kind], x_recv.at[lane, kind], me, to)

    def d_copy(lane, shift):
        src = win_ref.at[2 * lane] if lane else pay_ref
        return copy_to(
            src, win_ref.at[2 * lane + shift], d_send.at[lane], d_recv.at[lane], sibling, col
        )

    def on_core(which, also=None):
        mine = core == which
        return pl.when(mine if also is None else mine & also)

    far = (core == 1) & has(2) & feeds(2)
    number = 3 + jnp.minimum(2, chips - 1 - chip) + far.astype(jnp.int32)
    pl.semaphore_wait(barrier, number)
    for steps in (1, 2):

        @pl.when(feeds(steps))
        def _():
            y_copy(steps).start()

    @on_core(0)
    def _():
        d_copy(0, 1).start()

    def arrived(lane):
        y_copy(lane).wait_recv()
        if lane == 2:

            @pl.when(feeds(1))
            def _():
                y_copy(3).start()

            @pl.when(far)
            def _():
                y_copy(4).start()

        x_copy(lane, 0).start()
        x_copy(lane, 1).start()

    def relay(lane):
        x_copy(lane, 0).wait_recv()
        x_copy(lane, 2).start()
        x_copy(lane, 1).wait_recv()
        x_copy(lane, 3).start()

    def finish(lane):
        x_copy(lane, 2).wait_recv()
        x_copy(lane, 3).wait_recv()
        if lane < 4:

            @on_core(0)
            def _():
                d_copy(lane, 1).start()

            @on_core(1)
            def _():
                d_copy(lane, -1).start()

    def from_sibling(lane):
        @on_core(0)
        def _():
            d_copy(lane, -1).wait_recv()

        @on_core(1)
        def _():
            d_copy(lane, 1).wait_recv()

    scale = (CONTENT + ROTARY) ** (-0.5) * LOG2E
    for item in loads[:3]:
        item.wait()
    normed = rms_scale(latent_ref[...], query_gain_ref[...])
    content = jnp.dot(normed, content_ref[...], preferred_element_type=F32).astype(BF16)
    raw = jnp.dot(normed, rotary_weight_ref[...], preferred_element_type=F32)
    wide_cosine = jnp.concatenate([cosine] * 4, axis=0).T
    wide_sine = jnp.concatenate([-sine, sine, -sine, sine], axis=0).T
    lane_of = lax.broadcasted_iota(jnp.int32, (length, 2 * ROTARY), 1)
    for head in range(heads):
        cut = slice(head // 2 * 2 * ROTARY, (head // 2 + 1) * 2 * ROTARY)
        pair = rotate(raw[:, cut], wide_cosine, wide_sine)
        pair = jnp.where(lane_of // ROTARY == head % 2, pair, 0.0).astype(BF16)
        query[head, :, :CONTENT] = content[:, head * CONTENT : (head + 1) * CONTENT]
        query[head, :, CONTENT:] = pair
    highest[...] = jnp.full(highest.shape, MASKED, F32)
    denominator[...] = jnp.zeros(denominator.shape, F32)
    summed[...] = jnp.zeros(summed.shape, F32)
    loads[3].wait()
    value_turned[...] = value_ref[...].astype(F32).T.astype(BF16)
    loads[4].wait()
    anchor = me * length

    def absorb(slot, block_ref):
        shared = block_ref[:, :rank]
        turn = block_ref[:, rank:]
        keys = jnp.dot(shared, key_ref[...], preferred_element_type=F32).astype(BF16)
        values = lax.dot_general(
            value_turned[...], shared, (((1,), (1,)), ((), ())), preferred_element_type=F32
        ).astype(BF16)
        shape = (length, length)
        key_places = anchor - slot * length + lax.broadcasted_iota(jnp.int32, shape, 0)
        visible = key_places >= start_ref[...]
        if isinstance(slot, int) and slot == 0:
            visible = visible & (
                lax.broadcasted_iota(jnp.int32, shape, 0)
                <= lax.broadcasted_iota(jnp.int32, shape, 1)
            )
        for head in range(heads):
            cut = slice(head * CONTENT, (head + 1) * CONTENT)
            joined = jnp.concatenate([keys[:, cut], turn], axis=1)
            scores = lax.dot_general(
                joined, query[head], (((1,), (1,)), ((), ())), preferred_element_type=F32
            )
            scores = jnp.where(visible, scores * scale, MASKED)
            before = highest[head]
            after = jnp.maximum(before, jnp.max(scores, axis=0, keepdims=True))
            factor = jnp.exp2(before - after)
            weights = jnp.exp2(scores - after)
            highest[head] = after
            denominator[head] = denominator[head] * factor + jnp.sum(
                weights, axis=0, keepdims=True
            )
            summed[head] = summed[head] * factor + jnp.dot(
                values[cut, :], weights.astype(BF16), preferred_element_type=F32
            )

    def absorb_slot(slot):
        absorb(slot, win_ref.at[slot])

    absorb(0, pay_ref)

    @on_core(1)
    def _():
        d_copy(0, 1).wait_recv()
        absorb_slot(1)

    def absorb_sibling(lane):
        from_sibling(lane)
        absorb_slot(2 * lane - 1 + 2 * core)

    def steps_of(lane, *steps):
        @pl.when((core == 0) & has(4) if lane == 4 else has(lane))
        def _():
            for step in steps:
                step(lane)

    def absorb_lane(lane):
        absorb_slot(2 * lane if lane < 4 else 7)

    steps_of(1, arrived)
    steps_of(2, arrived)
    steps_of(1, relay)
    steps_of(2, relay)
    steps_of(1, finish, absorb_lane)
    steps_of(3, arrived)
    steps_of(4, arrived)
    steps_of(2, finish)
    steps_of(1, absorb_sibling)
    steps_of(2, absorb_lane)
    steps_of(3, relay)
    steps_of(4, relay)
    steps_of(2, absorb_sibling)
    steps_of(3, finish, absorb_lane)
    steps_of(4, finish, absorb_lane)
    steps_of(3, absorb_sibling)

    for head in range(heads):
        cut = slice(head * CONTENT, (head + 1) * CONTENT)
        attended[:, cut] = (summed[head] / denominator[head]).T.astype(BF16)
    loads[5].wait()

    size = length // CHUNKS
    half, piece = model // 4, model // 8
    bit = col // 2
    gray = lax.rem(col + bit, 2)
    near = (col + 1 - 2 * lax.rem(col, 2), ring - 1 - col)
    keep = (gray, bit)
    sub = (bit, gray)

    def part(chunk):
        return pl.ds(chunk * size, size)

    def half_at(side, which):
        return pl.multiple_of(side * (model // 2) + which * half, half)

    def piece_at(side, which, sub_which):
        return pl.multiple_of(side * (model // 2) + which * half + sub_which * piece, piece)

    def copy(kind, side, chunk, src, dst, partner):
        return copy_to(
            src, dst, send.at[kind, side, chunk], recv.at[kind, side, chunk], me, partner
        )

    def stage_one(side, chunk):
        return copy(
            0, side, chunk, term.at[side, part(chunk)], first.at[side, part(chunk)], near[side]
        )

    def stage_two(side, chunk):
        return copy(
            1, side, chunk, held.at[side, part(chunk)], second.at[side, part(chunk)], near[1 - side]
        )

    def gather(kind, side, chunk):
        which = 1 - sub[side] if kind == 4 else sub[side]
        ref = out_ref.at[part(chunk), pl.ds(piece_at(side, keep[side], which), piece)]
        return copy(kind, side, chunk, ref, ref, near[1 - side] if kind == 2 else near[side])

    def project(chunk, at, width):
        return jnp.dot(
            attended[part(chunk), :], weight_ref[:, pl.ds(at, width)], preferred_element_type=F32
        ).astype(BF16)

    for chunk in range(CHUNKS):
        for side in (0, 1):
            term[side, part(chunk), :] = project(chunk, half_at(side, 1 - keep[side]), half)
            stage_one(side, chunk).start()

    for chunk in range(CHUNKS):
        for side in (0, 1):
            theirs = pl.multiple_of((1 - sub[side]) * piece, piece)
            mine = project(chunk, piece_at(side, keep[side], 1 - sub[side]), piece)
            stage_one(side, chunk).wait_recv()
            held[side, part(chunk), :] = (
                mine.astype(F32) + first[side, part(chunk), pl.ds(theirs, piece)].astype(F32)
            ).astype(BF16)
            stage_two(side, chunk).start()

    for chunk in range(CHUNKS):
        for side in (0, 1):
            ours = pl.multiple_of(sub[side] * piece, piece)
            at = piece_at(side, keep[side], sub[side])
            mine = project(chunk, at, piece).astype(F32)
            mine = mine + first[side, part(chunk), pl.ds(ours, piece)].astype(F32)
            stage_two(side, chunk).wait_recv()
            out_ref[part(chunk), pl.ds(at, piece)] = (
                mine + second[side, part(chunk), :].astype(F32)
            ).astype(BF16)
            gather(2, side, chunk).start()
            gather(3, side, chunk).start()

    for chunk in range(CHUNKS):
        for side in (0, 1):
            gather(2, side, chunk).wait_recv()
            gather(4, side, chunk).start()

    for chunk in range(CHUNKS):
        for side in (0, 1):
            gather(3, side, chunk).wait_recv()
            gather(4, side, chunk).wait_recv()
            stage_one(side, chunk).wait_send()
            stage_two(side, chunk).wait_send()
            for kind in (2, 3, 4):
                gather(kind, side, chunk).wait_send()

    for steps in (1, 2, 3):

        @pl.when(feeds(steps) if steps < 3 else has(2) & feeds(1))
        def _():
            y_copy(steps).wait_send()

        @pl.when(has(steps))
        def _():
            for kind in range(4):
                x_copy(steps, kind).wait_send()
            d_copy(steps, -1).wait_send()

    @pl.when(far)
    def _():
        y_copy(4).wait_send()

    @on_core(0)
    def _():
        d_copy(0, 1).wait_send()

    @on_core(0, has(4))
    def _():
        for kind in range(4):
            x_copy(4, kind).wait_send()


def on_device(
    query_latent,
    shared_latent,
    rotary_key,
    document_start,
    query_gain,
    shared_gain,
    content_weight,
    rotary_weight,
    key_weight,
    value_weight,
    output_weight,
):
    length, query_rank = query_latent.shape
    rank = shared_latent.shape[1]
    model = output_weight.shape[1]
    heads = key_weight.shape[1] // CONTENT
    width = rank + 2 * ROTARY
    places = lax.axis_index("sp") * length + jnp.arange(length, dtype=jnp.int32)
    frequency = 1.0 / THETA ** (jnp.arange(0, ROTARY, 2, dtype=F32) / ROTARY)
    angles = frequency[:, None] * places.astype(F32)[None, :]
    vmem, dma = pltpu.VMEM, pltpu.SemaphoreType.DMA
    pinned = [
        pltpu.with_memory_space_constraint(item, pltpu.HBM)
        for item in (
            query_latent,
            shared_latent,
            rotary_key.T,
            document_start[None, :],
            jnp.cos(angles),
            jnp.sin(angles),
            query_gain[None, :],
            shared_gain[None, :],
            content_weight,
            rotary_weight,
            key_weight,
            value_weight,
            output_weight,
        )
    ]
    return pl.pallas_call(
        mixed_kernel,
        out_shape=jax.ShapeDtypeStruct((length, model), BF16),
        in_specs=[FAR] + [WHOLE] * 7 + [FAR] * 5,
        out_specs=WHOLE,
        scratch_shapes=[
            vmem((length, query_rank), BF16),
            vmem(content_weight.shape, BF16),
            vmem(rotary_weight.shape, BF16),
            vmem(key_weight.shape, BF16),
            vmem(value_weight.shape, BF16),
            vmem(output_weight.shape, BF16),
            vmem(value_weight.shape[::-1], BF16),
            vmem((length, width), BF16),
            vmem((SPAN, length, width), BF16),
            vmem((heads, length, 2 * CONTENT), BF16),
            vmem((heads, 1, length), F32),
            vmem((heads, 1, length), F32),
            vmem((heads, CONTENT, length), F32),
            vmem((length, heads * CONTENT), BF16),
            vmem((2, length, model // 4), BF16),
            vmem((2, length, model // 4), BF16),
            vmem((2, length, model // 8), BF16),
            vmem((2, length, model // 8), BF16),
            dma((6,)),
            dma((5,)),
            dma((5,)),
            dma((5, 4)),
            dma((5, 4)),
            dma((4,)),
            dma((4,)),
            dma((5, 2, CHUNKS)),
            dma((5, 2, CHUNKS)),
        ],
        compiler_params=pltpu.CompilerParams(
            collective_id=0, has_side_effects=True, vmem_limit_bytes=46 * 2**20
        ),
        name="mixed",
    )(

        *pinned,
    )


def solution(mesh):
    return jax.shard_map(
        on_device,
        mesh=mesh,
        in_specs=(
            P("sp", None),
            P("sp", None),
            P("sp", None),
            P("sp"),
            P(),
            P(),
            P(None, "tp"),
            P(None, "tp"),
            P(None, "tp"),
            P(None, "tp"),
            P("tp", None),
        ),
        out_specs=P("sp", None),
        check_vma=False,
    )
```

```python
import jax
import jax.numpy as jnp
from jax import lax
from jax.experimental import pallas as pl
from jax.experimental.pallas import tpu as pltpu
from jax.sharding import PartitionSpec as P

MESH = pl.DeviceIdType.MESH
CONTENT = 128
ROTARY = 64
SPAN = 8
NORM_EPS = 1e-06
THETA = 10000.0
MASKED = -1e30
LOG2E = 1.4426950408889634
F32 = jnp.float32
BF16 = jnp.bfloat16
WHOLE = pl.BlockSpec(memory_space=pltpu.VMEM)
FAR = pl.BlockSpec(memory_space=pltpu.HBM)
CHUNKS = 4


def copy_to(src, dst, send, recv, sp, tp):
    return pltpu.make_async_remote_copy(
        src_ref=src,
        dst_ref=dst,
        send_sem=send,
        recv_sem=recv,
        device_id={"sp": sp, "tp": tp},
        device_id_type=MESH,
    )


def rms_scale(entries, gain):
    entries = entries.astype(F32)
    mean = jnp.mean(entries * entries, axis=-1, keepdims=True)
    return (entries * lax.rsqrt(mean + NORM_EPS) * gain).astype(BF16)


def rotate(entries, cosine, sine):
    width = entries.shape[-1]
    lane = lax.broadcasted_iota(jnp.int32, entries.shape, 1)
    ahead = pltpu.roll(entries, width - ROTARY // 2, 1)
    behind = pltpu.roll(entries, ROTARY // 2, 1)
    other = jnp.where(lane % ROTARY < ROTARY // 2, ahead, behind)
    return entries * cosine + other * sine


def mixed_kernel(
    latent_hbm,
    shared_hbm,
    rotary_hbm,
    start_hbm,
    cos_hbm,
    sin_hbm,
    query_gain_hbm,
    shared_gain_hbm,
    content_hbm,
    rotary_weight_hbm,
    key_hbm,
    value_hbm,
    output_hbm,
    out_ref,
    shared_ref,
    rotary_ref,
    start_ref,
    cos_ref,
    sin_ref,
    query_gain_ref,
    shared_gain_ref,
    latent_ref,
    content_ref,
    rotary_weight_ref,
    key_ref,
    value_ref,
    weight_ref,
    value_turned,
    pay_ref,
    win_ref,
    query,
    highest,
    denominator,
    summed,
    attended,
    near_attended,
    near_weight,
    second,
    held,
    load_sem,
    y_send,
    y_recv,
    x_send,
    x_recv,
    d_send,
    d_recv,
    w_send,
    w_recv,
    s_send,
    s_recv,
    send,
    recv,
):
    count, ring = lax.axis_size("sp"), lax.axis_size("tp")
    me, col = lax.axis_index("sp"), lax.axis_index("tp")
    core = lax.rem(me, 2)
    chip, chips = me // 2, count // 2
    sibling = me + 1 - 2 * core
    east, west = lax.rem(col + 1, ring), lax.rem(col + ring - 1, ring)
    length, rank = shared_ref.shape
    heads = key_ref.shape[1] // CONTENT
    model = out_ref.shape[1]
    quarter, eighth = length // 4, length // 8
    size = length // CHUNKS
    half, piece = model // 4, model // 8
    bit = col // 2
    gray = lax.rem(col + bit, 2)
    near = (col + 1 - 2 * lax.rem(col, 2), ring - 1 - col)
    keep = (gray, bit)
    sub = (bit, gray)

    def piece_at(side, which, sub_which):
        return pl.multiple_of(side * (model // 2) + which * half + sub_which * piece, piece)

    def load(index, src, dst):
        return pltpu.make_async_copy(src, dst, load_sem.at[index])

    loads = [
        load(0, latent_hbm, latent_ref),
        load(1, content_hbm, content_ref),
        load(2, rotary_weight_hbm, rotary_weight_ref),
        load(3, value_hbm, value_ref),
        load(4, key_hbm, key_ref),
        load(5, output_hbm, weight_ref),
    ]
    small = [
        load(6, shared_hbm, shared_ref),
        load(7, rotary_hbm, rotary_ref),
        load(8, cos_hbm, cos_ref),
        load(9, sin_hbm, sin_ref),
        load(10, shared_gain_hbm, shared_gain_ref),
        load(11, query_gain_hbm, query_gain_ref),
        load(12, start_hbm, start_ref),
    ]
    for item in small + loads:
        item.start()

    barrier = pltpu.get_barrier_semaphore()

    def greet(sp, tp):
        pl.semaphore_signal(barrier, inc=1, device_id={"sp": sp, "tp": tp}, device_id_type=MESH)

    def has(steps):
        return chip >= steps

    def feeds(steps):
        return chip + steps < chips

    greet(me, east)
    greet(me, west)
    greet(sibling, col)
    for steps in (1, 2):

        @pl.when(has(steps))
        def _():
            greet(me - 2 * steps, col)

    @pl.when((core == 0) & has(4))
    def _():
        greet(me - 3, col)

    for item in small:
        item.wait()
    pay_ref[:, :rank] = rms_scale(shared_ref[...], shared_gain_ref[...])
    leading = rotary_ref[: ROTARY // 2, :].astype(F32)
    trailing = rotary_ref[ROTARY // 2 :, :].astype(F32)
    cosine, sine = cos_ref[...], sin_ref[...]
    turned = [leading * cosine - trailing * sine, leading * sine + trailing * cosine]
    pay_ref[:, rank:] = jnp.concatenate(turned * 2, axis=0).T.astype(BF16)

    def rows(owner, offset, size):
        return pl.ds(pl.multiple_of(owner * quarter + offset, eighth), size)

    def y_copy(steps):
        part = rows(col, 0, quarter)
        src = pay_ref.at[part] if steps < 3 else win_ref.at[4, part]
        slot, to = ((2, me + 2), (4, me + 4), (6, me + 2), (7, me + 3))[steps - 1]
        return copy_to(
            src, win_ref.at[slot, part], y_send.at[steps], y_recv.at[steps], to, col
        )

    def x_copy(lane, kind):
        slot = 2 * lane if lane < 4 else 7
        owner, offset, to = (
            (col, 0, east),
            (col, eighth, west),
            (west, 0, east),
            (east, eighth, west),
            (col, eighth, east),
            (col, 0, west),
        )[kind]
        part = rows(owner, offset, eighth)
        ref = win_ref.at[slot, part]
        return copy_to(ref, ref, x_send.at[lane, kind], x_recv.at[lane, kind], me, to)

    def d_copy(lane, shift):
        src = win_ref.at[2 * lane] if lane else pay_ref
        return copy_to(
            src, win_ref.at[2 * lane + shift], d_send.at[lane], d_recv.at[lane], sibling, col
        )

    def on_core(which, also=None):
        mine = core == which
        return pl.when(mine if also is None else mine & also)

    far = (core == 1) & has(2) & feeds(2)
    number = 3 + jnp.minimum(2, chips - 1 - chip) + far.astype(jnp.int32)
    pl.semaphore_wait(barrier, number)
    for steps in (2, 1):

        @pl.when(feeds(steps))
        def _():
            y_copy(steps).start()

    @on_core(0)
    def _():
        d_copy(0, 1).start()

    depth = weight_ref.shape[0] // 2
    core_rows = pl.ds(pl.multiple_of(core * depth, depth), depth)

    def w_copy(turn, side):
        at = piece_at(side, 1 - keep[side], 1 - sub[side] if turn == 0 else sub[side])
        return copy_to(
            output_hbm.at[core_rows, pl.ds(at, piece)],
            near_weight.at[turn, side, core_rows],
            w_send.at[turn, side],
            w_recv.at[turn, side],
            me,
            near[side],
        )

    def s_copy(turn, side):
        ref = near_weight.at[turn, side, core_rows]
        return copy_to(ref, ref, s_send.at[turn, side], s_recv.at[turn, side], sibling, col)

    def share(turn):
        for side in (0, 1):
            w_copy(turn, side).wait_recv()
            s_copy(turn, side).start()

    for side in (0, 1):
        w_copy(0, side).start()

    def arrived(lane):
        y_copy(lane).wait_recv()
        if lane == 2:

            @pl.when(feeds(1))
            def _():
                y_copy(3).start()

            @pl.when(far)
            def _():
                y_copy(4).start()

        for kind in (0, 1, 4, 5):
            x_copy(lane, kind).start()

    def relay(lane):
        x_copy(lane, 0).wait_recv()
        x_copy(lane, 2).start()
        x_copy(lane, 1).wait_recv()
        x_copy(lane, 3).start()

    def finish(lane):
        for kind in (4, 5, 2, 3):
            x_copy(lane, kind).wait_recv()
        if lane < 4:

            @on_core(0)
            def _():
                d_copy(lane, 1).start()

            @on_core(1)
            def _():
                d_copy(lane, -1).start()

    def from_sibling(lane):
        @on_core(0)
        def _():
            d_copy(lane, -1).wait_recv()

        @on_core(1)
        def _():
            d_copy(lane, 1).wait_recv()

    scale = (CONTENT + ROTARY) ** (-0.5) * LOG2E
    for item in loads[:3]:
        item.wait()
    normed = rms_scale(latent_ref[...], query_gain_ref[...])
    content = jnp.dot(normed, content_ref[...], preferred_element_type=F32).astype(BF16)
    raw = jnp.dot(normed, rotary_weight_ref[...], preferred_element_type=F32)
    wide_cosine = jnp.concatenate([cosine] * 4, axis=0).T
    wide_sine = jnp.concatenate([-sine, sine, -sine, sine], axis=0).T
    lane_of = lax.broadcasted_iota(jnp.int32, (length, 2 * ROTARY), 1)
    for head in range(heads):
        cut = slice(head // 2 * 2 * ROTARY, (head // 2 + 1) * 2 * ROTARY)
        pair = rotate(raw[:, cut], wide_cosine, wide_sine)
        pair = jnp.where(lane_of // ROTARY == head % 2, pair, 0.0).astype(BF16)
        query[head, :, :CONTENT] = content[:, head * CONTENT : (head + 1) * CONTENT]
        query[head, :, CONTENT:] = pair
    highest[...] = jnp.full(highest.shape, MASKED, F32)
    denominator[...] = jnp.zeros(denominator.shape, F32)
    summed[...] = jnp.zeros(summed.shape, F32)
    loads[3].wait()
    value_turned[...] = value_ref[...].astype(F32).T.astype(BF16)
    loads[4].wait()
    anchor = me * length

    def absorb(slot, block_ref):
        shared = block_ref[:, :rank]
        turn = block_ref[:, rank:]
        keys = jnp.dot(shared, key_ref[...], preferred_element_type=F32).astype(BF16)
        values = lax.dot_general(
            value_turned[...], shared, (((1,), (1,)), ((), ())), preferred_element_type=F32
        ).astype(BF16)
        shape = (length, length)
        key_places = anchor - slot * length + lax.broadcasted_iota(jnp.int32, shape, 0)
        visible = key_places >= start_ref[...]
        if isinstance(slot, int) and slot == 0:
            visible = visible & (
                lax.broadcasted_iota(jnp.int32, shape, 0)
                <= lax.broadcasted_iota(jnp.int32, shape, 1)
            )
        for head in range(heads):
            cut = slice(head * CONTENT, (head + 1) * CONTENT)
            joined = jnp.concatenate([keys[:, cut], turn], axis=1)
            scores = lax.dot_general(
                joined, query[head], (((1,), (1,)), ((), ())), preferred_element_type=F32
            )
            scores = jnp.where(visible, scores * scale, MASKED)
            before = highest[head]
            after = jnp.maximum(before, jnp.max(scores, axis=0, keepdims=True))
            factor = jnp.exp2(before - after)
            weights = jnp.exp2(scores - after)
            highest[head] = after
            denominator[head] = denominator[head] * factor + jnp.sum(
                weights, axis=0, keepdims=True
            )
            summed[head] = summed[head] * factor + jnp.dot(
                values[cut, :], weights.astype(BF16), preferred_element_type=F32
            )

    def absorb_slot(slot):
        absorb(slot, win_ref.at[slot])

    absorb(0, pay_ref)

    @on_core(1)
    def _():
        d_copy(0, 1).wait_recv()
        absorb_slot(1)

    def absorb_sibling(lane):
        from_sibling(lane)
        absorb_slot(2 * lane - 1 + 2 * core)

    def steps_of(lane, *steps):
        @pl.when((core == 0) & has(4) if lane == 4 else has(lane))
        def _():
            for step in steps:
                step(lane)

    def absorb_lane(lane):
        absorb_slot(2 * lane if lane < 4 else 7)

    steps_of(2, arrived)
    steps_of(1, arrived)
    steps_of(2, relay)
    steps_of(1, relay)
    steps_of(3, arrived)
    steps_of(4, arrived)
    steps_of(2, finish, absorb_lane)
    steps_of(1, finish)
    steps_of(3, relay)
    steps_of(4, relay)
    for side in (0, 1):
        w_copy(1, side).start()
    steps_of(1, absorb_lane)
    share(0)
    steps_of(2, absorb_sibling)
    steps_of(3, finish)
    steps_of(1, absorb_sibling)
    steps_of(3, absorb_lane)
    steps_of(4, finish, absorb_lane)
    steps_of(3, absorb_sibling)

    for head in range(heads):
        cut = slice(head * CONTENT, (head + 1) * CONTENT)
        attended[:, cut] = (summed[head] / denominator[head]).T.astype(BF16)

    def part(chunk):
        return pl.ds(chunk * size, size)

    def copy(kind, side, chunk, src, dst, partner):
        return copy_to(
            src, dst, send.at[kind, side, chunk], recv.at[kind, side, chunk], me, partner
        )

    def stage_one(side, chunk):
        return copy(
            0,
            side,
            chunk,
            attended.at[part(chunk)],
            near_attended.at[side, part(chunk)],
            near[side],
        )

    def stage_two(side, chunk):
        return copy(
            1, side, chunk, held.at[side, part(chunk)], second.at[side, part(chunk)], near[1 - side]
        )

    def gather(kind, side, chunk):
        which = 1 - sub[side] if kind == 4 else sub[side]
        ref = out_ref.at[part(chunk), pl.ds(piece_at(side, keep[side], which), piece)]
        return copy(kind, side, chunk, ref, ref, near[1 - side] if kind == 2 else near[side])

    def project(chunk, at):
        return (
            jnp.dot(
                attended[part(chunk), :],
                weight_ref[:, pl.ds(at, piece)],
                preferred_element_type=F32,
            )
            .astype(BF16)
            .astype(F32)
        )

    def project_near(turn, side, chunk):
        return (
            jnp.dot(
                near_attended[side, part(chunk), :],
                near_weight[turn, side],
                preferred_element_type=F32,
            )
            .astype(BF16)
            .astype(F32)
        )

    for chunk in range(CHUNKS):
        for side in (0, 1):
            stage_one(side, chunk).start()
    share(1)
    loads[5].wait()
    for side in (0, 1):
        s_copy(0, side).wait_recv()

    for chunk in range(CHUNKS):
        for side in (0, 1):
            mine = project(chunk, piece_at(side, keep[side], 1 - sub[side]))
            stage_one(side, chunk).wait_recv()
            held[side, part(chunk), :] = (mine + project_near(0, side, chunk)).astype(BF16)
            stage_two(side, chunk).start()

    for side in (0, 1):
        s_copy(1, side).wait_recv()

    for chunk in range(CHUNKS):
        for side in (0, 1):
            at = piece_at(side, keep[side], sub[side])
            mine = project(chunk, at) + project_near(1, side, chunk)
            stage_two(side, chunk).wait_recv()
            out_ref[part(chunk), pl.ds(at, piece)] = (
                mine + second[side, part(chunk), :].astype(F32)
            ).astype(BF16)
            gather(2, side, chunk).start()
            gather(3, side, chunk).start()

    for chunk in range(CHUNKS):
        for side in (0, 1):
            gather(2, side, chunk).wait_recv()
            gather(4, side, chunk).start()

    for chunk in range(CHUNKS):
        for side in (0, 1):
            gather(3, side, chunk).wait_recv()
            gather(4, side, chunk).wait_recv()
            stage_one(side, chunk).wait_send()
            stage_two(side, chunk).wait_send()
            for kind in (2, 3, 4):
                gather(kind, side, chunk).wait_send()

    for turn in (0, 1):
        for side in (0, 1):
            w_copy(turn, side).wait_send()
            s_copy(turn, side).wait_send()
    for steps in (1, 2, 3):

        @pl.when(feeds(steps) if steps < 3 else has(2) & feeds(1))
        def _():
            y_copy(steps).wait_send()

        @pl.when(has(steps))
        def _():
            for kind in range(6):
                x_copy(steps, kind).wait_send()
            d_copy(steps, -1).wait_send()

    @pl.when(far)
    def _():
        y_copy(4).wait_send()

    @on_core(0)
    def _():
        d_copy(0, 1).wait_send()

    @on_core(0, has(4))
    def _():
        for kind in range(6):
            x_copy(4, kind).wait_send()


def on_device(
    query_latent,
    shared_latent,
    rotary_key,
    document_start,
    query_gain,
    shared_gain,
    content_weight,
    rotary_weight,
    key_weight,
    value_weight,
    output_weight,
):
    length, query_rank = query_latent.shape
    rank = shared_latent.shape[1]
    model = output_weight.shape[1]
    heads = key_weight.shape[1] // CONTENT
    width = rank + 2 * ROTARY
    places = lax.axis_index("sp") * length + jnp.arange(length, dtype=jnp.int32)
    frequency = 1.0 / THETA ** (jnp.arange(0, ROTARY, 2, dtype=F32) / ROTARY)
    angles = frequency[:, None] * places.astype(F32)[None, :]
    vmem, dma = pltpu.VMEM, pltpu.SemaphoreType.DMA
    pinned = [
        pltpu.with_memory_space_constraint(item, pltpu.HBM)
        for item in (
            query_latent,
            shared_latent,
            rotary_key.T,
            document_start[None, :],
            jnp.cos(angles),
            jnp.sin(angles),
            query_gain[None, :],
            shared_gain[None, :],
            content_weight,
            rotary_weight,
            key_weight,
            value_weight,
            output_weight,
        )
    ]
    return pl.pallas_call(
        mixed_kernel,
        out_shape=jax.ShapeDtypeStruct((length, model), BF16),
        in_specs=[FAR] * 13,
        out_specs=WHOLE,
        scratch_shapes=[
            vmem((length, rank), BF16),
            vmem((ROTARY, length), BF16),
            vmem((1, length), jnp.int32),
            vmem((ROTARY // 2, length), F32),
            vmem((ROTARY // 2, length), F32),
            vmem((1, query_rank), F32),
            vmem((1, rank), F32),
            vmem((length, query_rank), BF16),
            vmem(content_weight.shape, BF16),
            vmem(rotary_weight.shape, BF16),
            vmem(key_weight.shape, BF16),
            vmem(value_weight.shape, BF16),
            vmem(output_weight.shape, BF16),
            vmem(value_weight.shape[::-1], BF16),
            vmem((length, width), BF16),
            vmem((SPAN, length, width), BF16),
            vmem((heads, length, 2 * CONTENT), BF16),
            vmem((heads, 1, length), F32),
            vmem((heads, 1, length), F32),
            vmem((heads, CONTENT, length), F32),
            vmem((length, heads * CONTENT), BF16),
            vmem((2, length, heads * CONTENT), BF16),
            vmem((2, 2, output_weight.shape[0], model // 8), BF16),
            vmem((2, length, model // 8), BF16),
            vmem((2, length, model // 8), BF16),
            dma((13,)),
            dma((5,)),
            dma((5,)),
            dma((5, 6)),
            dma((5, 6)),
            dma((4,)),
            dma((4,)),
            dma((2, 2)),
            dma((2, 2)),
            dma((2, 2)),
            dma((2, 2)),
            dma((5, 2, CHUNKS)),
            dma((5, 2, CHUNKS)),
        ],
        compiler_params=pltpu.CompilerParams(
            collective_id=0, has_side_effects=True, vmem_limit_bytes=46 * 2**20
        ),
        name="mixed",
    )(

        *pinned,
    )


def solution(mesh):
    return jax.shard_map(
        on_device,
        mesh=mesh,
        in_specs=(
            P("sp", None),
            P("sp", None),
            P("sp", None),
            P("sp"),
            P(),
            P(),
            P(None, "tp"),
            P(None, "tp"),
            P(None, "tp"),
            P(None, "tp"),
            P("tp", None),
        ),
        out_specs=P("sp", None),
        check_vma=False,
    )
```

```python
import jax
import jax.numpy as jnp
from jax import lax
from jax.experimental import pallas as pl
from jax.experimental.pallas import tpu as pltpu
from jax.sharding import PartitionSpec as P

MESH = pl.DeviceIdType.MESH
CONTENT = 128
ROTARY = 64
SPAN = 8
NORM_EPS = 1e-06
THETA = 10000.0
MASKED = -1e30
LOG2E = 1.4426950408889634
F32 = jnp.float32
BF16 = jnp.bfloat16
WHOLE = pl.BlockSpec(memory_space=pltpu.VMEM)
FAR = pl.BlockSpec(memory_space=pltpu.HBM)
CHUNKS = 4


def copy_to(src, dst, send, recv, sp, tp):
    return pltpu.make_async_remote_copy(
        src_ref=src,
        dst_ref=dst,
        send_sem=send,
        recv_sem=recv,
        device_id={"sp": sp, "tp": tp},
        device_id_type=MESH,
    )


def rms_scale(entries, gain):
    entries = entries.astype(F32)
    mean = jnp.mean(entries * entries, axis=-1, keepdims=True)
    return (entries * lax.rsqrt(mean + NORM_EPS) * gain).astype(BF16)


def rotate(entries, cosine, sine):
    width = entries.shape[-1]
    lane = lax.broadcasted_iota(jnp.int32, entries.shape, 1)
    ahead = pltpu.roll(entries, width - ROTARY // 2, 1)
    behind = pltpu.roll(entries, ROTARY // 2, 1)
    other = jnp.where(lane % ROTARY < ROTARY // 2, ahead, behind)
    return entries * cosine + other * sine


def mixed_kernel(
    latent_hbm,
    shared_hbm,
    rotary_hbm,
    start_hbm,
    cos_hbm,
    sin_hbm,
    query_gain_hbm,
    shared_gain_hbm,
    content_hbm,
    rotary_weight_hbm,
    key_hbm,
    value_hbm,
    output_hbm,
    out_ref,
    shared_ref,
    rotary_ref,
    start_ref,
    cos_ref,
    sin_ref,
    query_gain_ref,
    shared_gain_ref,
    latent_ref,
    content_ref,
    rotary_weight_ref,
    key_ref,
    value_ref,
    weight_ref,
    value_turned,
    pay_ref,
    win_ref,
    query,
    highest,
    denominator,
    summed,
    attended,
    near_attended,
    near_weight,
    second,
    held,
    load_sem,
    y_send,
    y_recv,
    x_send,
    x_recv,
    d_send,
    d_recv,
    w_send,
    w_recv,
    s_send,
    s_recv,
    send,
    recv,
):
    count, ring = lax.axis_size("sp"), lax.axis_size("tp")
    me, col = lax.axis_index("sp"), lax.axis_index("tp")
    core = lax.rem(me, 2)
    chip, chips = me // 2, count // 2
    sibling = me + 1 - 2 * core
    east, west = lax.rem(col + 1, ring), lax.rem(col + ring - 1, ring)
    length, rank = shared_ref.shape
    heads = key_ref.shape[1] // CONTENT
    model = out_ref.shape[1]
    quarter, eighth = length // 4, length // 8
    size = length // CHUNKS
    half, piece = model // 4, model // 8
    bit = col // 2
    gray = lax.rem(col + bit, 2)
    near = (col + 1 - 2 * lax.rem(col, 2), ring - 1 - col)
    keep = (gray, bit)
    sub = (bit, gray)

    def piece_at(side, which, sub_which):
        return pl.multiple_of(side * (model // 2) + which * half + sub_which * piece, piece)

    def load(index, src, dst):
        return pltpu.make_async_copy(src, dst, load_sem.at[index])

    loads = [
        load(0, latent_hbm, latent_ref),
        load(1, content_hbm, content_ref),
        load(2, rotary_weight_hbm, rotary_weight_ref),
        load(3, value_hbm, value_ref),
        load(4, key_hbm, key_ref),
        load(5, output_hbm, weight_ref),
    ]
    small = [
        load(6, shared_hbm, shared_ref),
        load(7, rotary_hbm, rotary_ref),
        load(8, cos_hbm, cos_ref),
        load(9, sin_hbm, sin_ref),
        load(10, shared_gain_hbm, shared_gain_ref),
        load(11, query_gain_hbm, query_gain_ref),
        load(12, start_hbm, start_ref),
    ]
    for item in small + loads:
        item.start()

    barrier = pltpu.get_barrier_semaphore()

    def greet(sp, tp):
        pl.semaphore_signal(barrier, inc=1, device_id={"sp": sp, "tp": tp}, device_id_type=MESH)

    def has(steps):
        return chip >= steps

    def feeds(steps):
        return chip + steps < chips

    greet(me, east)
    greet(me, west)
    greet(sibling, col)
    for steps in (1, 2):

        @pl.when(has(steps))
        def _():
            greet(me - 2 * steps, col)

    @pl.when((core == 0) & has(4))
    def _():
        greet(me - 3, col)

    for item in small:
        item.wait()
    pay_ref[:, :rank] = rms_scale(shared_ref[...], shared_gain_ref[...])
    leading = rotary_ref[: ROTARY // 2, :].astype(F32)
    trailing = rotary_ref[ROTARY // 2 :, :].astype(F32)
    cosine, sine = cos_ref[...], sin_ref[...]
    turned = [leading * cosine - trailing * sine, leading * sine + trailing * cosine]
    pay_ref[:, rank:] = jnp.concatenate(turned * 2, axis=0).T.astype(BF16)

    def rows(owner, offset, size):
        return pl.ds(pl.multiple_of(owner * quarter + offset, eighth), size)

    def y_copy(steps):
        part = rows(col, 0, quarter)
        src = pay_ref.at[part] if steps < 3 else win_ref.at[4, part]
        slot, to = ((2, me + 2), (4, me + 4), (6, me + 2), (7, me + 3))[steps - 1]
        return copy_to(
            src, win_ref.at[slot, part], y_send.at[steps], y_recv.at[steps], to, col
        )

    def x_copy(lane, kind):
        slot = 2 * lane if lane < 4 else 7
        owner, offset, to = (
            (col, 0, east),
            (col, eighth, west),
            (west, 0, east),
            (east, eighth, west),
            (col, eighth, east),
            (col, 0, west),
        )[kind]
        part = rows(owner, offset, eighth)
        ref = win_ref.at[slot, part]
        return copy_to(ref, ref, x_send.at[lane, kind], x_recv.at[lane, kind], me, to)

    def d_copy(lane, shift):
        src = win_ref.at[2 * lane] if lane else pay_ref
        return copy_to(
            src, win_ref.at[2 * lane + shift], d_send.at[lane], d_recv.at[lane], sibling, col
        )

    def on_core(which, also=None):
        mine = core == which
        return pl.when(mine if also is None else mine & also)

    far = (core == 1) & has(2) & feeds(2)
    number = 3 + jnp.minimum(2, chips - 1 - chip) + far.astype(jnp.int32)
    pl.semaphore_wait(barrier, number)
    for steps in (2, 1):

        @pl.when(feeds(steps))
        def _():
            y_copy(steps).start()

    @on_core(0)
    def _():
        d_copy(0, 1).start()

    depth = weight_ref.shape[0] // 2
    core_rows = pl.ds(pl.multiple_of(core * depth, depth), depth)

    def w_copy(turn, side):
        at = piece_at(side, 1 - keep[side], 1 - sub[side] if turn == 0 else sub[side])
        return copy_to(
            output_hbm.at[core_rows, pl.ds(at, piece)],
            near_weight.at[turn, side, core_rows],
            w_send.at[turn, side],
            w_recv.at[turn, side],
            me,
            near[side],
        )

    def s_copy(turn, side):
        ref = near_weight.at[turn, side, core_rows]
        return copy_to(ref, ref, s_send.at[turn, side], s_recv.at[turn, side], sibling, col)

    def share(turn):
        for side in (0, 1):
            w_copy(turn, side).wait_recv()
            s_copy(turn, side).start()

    for side in (0, 1):
        w_copy(0, side).start()

    def arrived(lane):
        y_copy(lane).wait_recv()
        if lane == 2:

            @pl.when(feeds(1))
            def _():
                y_copy(3).start()

            @pl.when(far)
            def _():
                y_copy(4).start()

        for kind in (0, 1, 4, 5):
            x_copy(lane, kind).start()

    def relay(lane):
        x_copy(lane, 0).wait_recv()
        x_copy(lane, 2).start()
        x_copy(lane, 1).wait_recv()
        x_copy(lane, 3).start()

    def finish(lane):
        for kind in (4, 5, 2, 3):
            x_copy(lane, kind).wait_recv()
        if lane < 4:

            @on_core(0)
            def _():
                d_copy(lane, 1).start()

            @on_core(1)
            def _():
                d_copy(lane, -1).start()

    def from_sibling(lane):
        @on_core(0)
        def _():
            d_copy(lane, -1).wait_recv()

        @on_core(1)
        def _():
            d_copy(lane, 1).wait_recv()

    scale = (CONTENT + ROTARY) ** (-0.5) * LOG2E
    for item in loads[:3]:
        item.wait()
    normed = rms_scale(latent_ref[...], query_gain_ref[...])
    content = jnp.dot(normed, content_ref[...], preferred_element_type=F32).astype(BF16)
    raw = jnp.dot(normed, rotary_weight_ref[...], preferred_element_type=F32)
    wide_cosine = jnp.concatenate([cosine] * 4, axis=0).T
    wide_sine = jnp.concatenate([-sine, sine, -sine, sine], axis=0).T
    lane_of = lax.broadcasted_iota(jnp.int32, (length, 2 * ROTARY), 1)
    for head in range(heads):
        cut = slice(head // 2 * 2 * ROTARY, (head // 2 + 1) * 2 * ROTARY)
        pair = rotate(raw[:, cut], wide_cosine, wide_sine)
        pair = jnp.where(lane_of // ROTARY == head % 2, pair, 0.0).astype(BF16)
        query[head, :, :CONTENT] = content[:, head * CONTENT : (head + 1) * CONTENT]
        query[head, :, CONTENT:] = pair
    highest[...] = jnp.full(highest.shape, MASKED, F32)
    denominator[...] = jnp.zeros(denominator.shape, F32)
    summed[...] = jnp.zeros(summed.shape, F32)
    loads[3].wait()
    value_turned[...] = value_ref[...].astype(F32).T.astype(BF16)
    loads[4].wait()
    anchor = me * length

    def absorb(slot, block_ref):
        shared = block_ref[:, :rank]
        turn = block_ref[:, rank:]
        keys = jnp.dot(shared, key_ref[...], preferred_element_type=F32).astype(BF16)
        values = lax.dot_general(
            value_turned[...], shared, (((1,), (1,)), ((), ())), preferred_element_type=F32
        ).astype(BF16)
        shape = (length, length)
        key_places = anchor - slot * length + lax.broadcasted_iota(jnp.int32, shape, 0)
        visible = key_places >= start_ref[...]
        if isinstance(slot, int) and slot == 0:
            visible = visible & (
                lax.broadcasted_iota(jnp.int32, shape, 0)
                <= lax.broadcasted_iota(jnp.int32, shape, 1)
            )
        for head in range(heads):
            cut = slice(head * CONTENT, (head + 1) * CONTENT)
            joined = jnp.concatenate([keys[:, cut], turn], axis=1)
            scores = lax.dot_general(
                joined, query[head], (((1,), (1,)), ((), ())), preferred_element_type=F32
            )
            scores = jnp.where(visible, scores * scale, MASKED)
            before = highest[head]
            after = jnp.maximum(before, jnp.max(scores, axis=0, keepdims=True))
            factor = jnp.exp2(before - after)
            weights = jnp.exp2(scores - after)
            highest[head] = after
            denominator[head] = denominator[head] * factor + jnp.sum(
                weights, axis=0, keepdims=True
            )
            summed[head] = summed[head] * factor + jnp.dot(
                values[cut, :], weights.astype(BF16), preferred_element_type=F32
            )

    def absorb_slot(slot):
        absorb(slot, win_ref.at[slot])

    absorb(0, pay_ref)

    @on_core(1)
    def _():
        d_copy(0, 1).wait_recv()
        absorb_slot(1)

    def absorb_sibling(lane):
        from_sibling(lane)
        absorb_slot(2 * lane - 1 + 2 * core)

    def steps_of(lane, *steps):
        @pl.when((core == 0) & has(4) if lane == 4 else has(lane))
        def _():
            for step in steps:
                step(lane)

    def absorb_lane(lane):
        absorb_slot(2 * lane if lane < 4 else 7)

    steps_of(2, arrived)
    steps_of(1, arrived)
    steps_of(2, relay)
    steps_of(1, relay)
    steps_of(3, arrived)
    steps_of(4, arrived)
    steps_of(2, finish, absorb_lane)
    steps_of(1, finish, absorb_lane)
    steps_of(3, relay)
    steps_of(2, absorb_sibling)
    steps_of(4, relay)
    for side in (0, 1):
        w_copy(1, side).start()
    share(0)
    steps_of(1, absorb_sibling)
    steps_of(3, finish, absorb_lane)
    steps_of(4, finish, absorb_lane)
    steps_of(3, absorb_sibling)

    for head in range(heads):
        cut = slice(head * CONTENT, (head + 1) * CONTENT)
        attended[:, cut] = (summed[head] / denominator[head]).T.astype(BF16)

    def part(chunk):
        return pl.ds(chunk * size, size)

    def copy(kind, side, chunk, src, dst, partner):
        return copy_to(
            src, dst, send.at[kind, side, chunk], recv.at[kind, side, chunk], me, partner
        )

    def stage_one(side, chunk):
        return copy(
            0,
            side,
            chunk,
            attended.at[part(chunk)],
            near_attended.at[side, part(chunk)],
            near[side],
        )

    def stage_two(side, chunk):
        return copy(
            1, side, chunk, held.at[side, part(chunk)], second.at[side, part(chunk)], near[1 - side]
        )

    def gather(kind, side, chunk):
        which = 1 - sub[side] if kind == 4 else sub[side]
        ref = out_ref.at[part(chunk), pl.ds(piece_at(side, keep[side], which), piece)]
        return copy(kind, side, chunk, ref, ref, near[1 - side] if kind == 2 else near[side])

    def project(chunk, at):
        return (
            jnp.dot(
                attended[part(chunk), :],
                weight_ref[:, pl.ds(at, piece)],
                preferred_element_type=F32,
            )
            .astype(BF16)
            .astype(F32)
        )

    def project_near(turn, side, chunk):
        return (
            jnp.dot(
                near_attended[side, part(chunk), :],
                near_weight[turn, side],
                preferred_element_type=F32,
            )
            .astype(BF16)
            .astype(F32)
        )

    for chunk in range(CHUNKS):
        for side in (0, 1):
            stage_one(side, chunk).start()
    share(1)
    loads[5].wait()
    for side in (0, 1):
        s_copy(0, side).wait_recv()

    for chunk in range(CHUNKS):
        for side in (0, 1):
            mine = project(chunk, piece_at(side, keep[side], 1 - sub[side]))
            stage_one(side, chunk).wait_recv()
            held[side, part(chunk), :] = (mine + project_near(0, side, chunk)).astype(BF16)
            stage_two(side, chunk).start()

    for side in (0, 1):
        s_copy(1, side).wait_recv()

    for chunk in range(CHUNKS):
        for side in (0, 1):
            at = piece_at(side, keep[side], sub[side])
            mine = project(chunk, at) + project_near(1, side, chunk)
            stage_two(side, chunk).wait_recv()
            out_ref[part(chunk), pl.ds(at, piece)] = (
                mine + second[side, part(chunk), :].astype(F32)
            ).astype(BF16)
            gather(2, side, chunk).start()
            gather(3, side, chunk).start()

    for chunk in range(CHUNKS):
        for side in (0, 1):
            gather(2, side, chunk).wait_recv()
            gather(4, side, chunk).start()

    for chunk in range(CHUNKS):
        for side in (0, 1):
            gather(3, side, chunk).wait_recv()
            gather(4, side, chunk).wait_recv()
            stage_one(side, chunk).wait_send()
            stage_two(side, chunk).wait_send()
            for kind in (2, 3, 4):
                gather(kind, side, chunk).wait_send()

    for turn in (0, 1):
        for side in (0, 1):
            w_copy(turn, side).wait_send()
            s_copy(turn, side).wait_send()
    for steps in (1, 2, 3):

        @pl.when(feeds(steps) if steps < 3 else has(2) & feeds(1))
        def _():
            y_copy(steps).wait_send()

        @pl.when(has(steps))
        def _():
            for kind in range(6):
                x_copy(steps, kind).wait_send()
            d_copy(steps, -1).wait_send()

    @pl.when(far)
    def _():
        y_copy(4).wait_send()

    @on_core(0)
    def _():
        d_copy(0, 1).wait_send()

    @on_core(0, has(4))
    def _():
        for kind in range(6):
            x_copy(4, kind).wait_send()


def on_device(
    query_latent,
    shared_latent,
    rotary_key,
    document_start,
    query_gain,
    shared_gain,
    content_weight,
    rotary_weight,
    key_weight,
    value_weight,
    output_weight,
):
    length, query_rank = query_latent.shape
    rank = shared_latent.shape[1]
    model = output_weight.shape[1]
    heads = key_weight.shape[1] // CONTENT
    width = rank + 2 * ROTARY
    places = lax.axis_index("sp") * length + jnp.arange(length, dtype=jnp.int32)
    frequency = 1.0 / THETA ** (jnp.arange(0, ROTARY, 2, dtype=F32) / ROTARY)
    angles = frequency[:, None] * places.astype(F32)[None, :]
    vmem, dma = pltpu.VMEM, pltpu.SemaphoreType.DMA
    pinned = [
        pltpu.with_memory_space_constraint(item, pltpu.HBM)
        for item in (
            query_latent,
            shared_latent,
            rotary_key.T,
            document_start[None, :],
            jnp.cos(angles),
            jnp.sin(angles),
            query_gain[None, :],
            shared_gain[None, :],
            content_weight,
            rotary_weight,
            key_weight,
            value_weight,
            output_weight,
        )
    ]
    return pl.pallas_call(
        mixed_kernel,
        out_shape=jax.ShapeDtypeStruct((length, model), BF16),
        in_specs=[FAR] * 13,
        out_specs=WHOLE,
        scratch_shapes=[
            vmem((length, rank), BF16),
            vmem((ROTARY, length), BF16),
            vmem((1, length), jnp.int32),
            vmem((ROTARY // 2, length), F32),
            vmem((ROTARY // 2, length), F32),
            vmem((1, query_rank), F32),
            vmem((1, rank), F32),
            vmem((length, query_rank), BF16),
            vmem(content_weight.shape, BF16),
            vmem(rotary_weight.shape, BF16),
            vmem(key_weight.shape, BF16),
            vmem(value_weight.shape, BF16),
            vmem(output_weight.shape, BF16),
            vmem(value_weight.shape[::-1], BF16),
            vmem((length, width), BF16),
            vmem((SPAN, length, width), BF16),
            vmem((heads, length, 2 * CONTENT), BF16),
            vmem((heads, 1, length), F32),
            vmem((heads, 1, length), F32),
            vmem((heads, CONTENT, length), F32),
            vmem((length, heads * CONTENT), BF16),
            vmem((2, length, heads * CONTENT), BF16),
            vmem((2, 2, output_weight.shape[0], model // 8), BF16),
            vmem((2, length, model // 8), BF16),
            vmem((2, length, model // 8), BF16),
            dma((13,)),
            dma((5,)),
            dma((5,)),
            dma((5, 6)),
            dma((5, 6)),
            dma((4,)),
            dma((4,)),
            dma((2, 2)),
            dma((2, 2)),
            dma((2, 2)),
            dma((2, 2)),
            dma((5, 2, CHUNKS)),
            dma((5, 2, CHUNKS)),
        ],
        compiler_params=pltpu.CompilerParams(
            collective_id=0, has_side_effects=True, vmem_limit_bytes=46 * 2**20
        ),
        name="mixed",
    )(

        *pinned,
    )


def solution(mesh):
    return jax.shard_map(
        on_device,
        mesh=mesh,
        in_specs=(
            P("sp", None),
            P("sp", None),
            P("sp", None),
            P("sp"),
            P(),
            P(),
            P(None, "tp"),
            P(None, "tp"),
            P(None, "tp"),
            P(None, "tp"),
            P("tp", None),
        ),
        out_specs=P("sp", None),
        check_vma=False,
    )
```
